256 devices in a mesh: sp: 32 (over z, x), tp: 8 (over y, core).
Axes of the slice: x: 4, y: 4, z: 8, core: 2. Of those that a mesh axis runs over, the one named last changes fastest.
Arguments:
- x_resid: bfloat16 [8192, 2048], P(('sp', 'tp')), may hold values from -3 to 3
- query_proj: bfloat16 [8192, 2048], P('sp', 'tp'), may hold values from -6 to 6
- projected_key_heads: bfloat16 [8192, 1024], P('sp', 'tp'), may hold values from -6 to 6
- projected_value_heads: bfloat16 [8192, 1024], P('sp', 'tp'), may hold values from -6 to 6
- query_gain: float32 [128], replicated, may hold values from 1.3 to 6.5
- key_norm_gain: float32 [128], replicated, may hold values from 1.3 to 6.5
- out_weight: bfloat16 [2048, 2048], P('tp'), may hold values from -0.125 to 0.125
- ffn_gain: float32 [2048], replicated, may hold values from 0.1 to 1.9
- routing: int32 [8192, 2], P(('sp', 'tp')), may hold values from 0 to 31, all different within a row; in each aligned block of 32 rows (0 to 31, 32 to 63, ...) at most 4 rows name the same one
- route_scores: float32 [8192, 2], P(('sp', 'tp')), may hold values from -6 to 6
- expert_gate: bfloat16 [32, 2048, 4096], P('sp', None, 'tp'), may hold values from -0.125 to 0.125
- expert_up: bfloat16 [32, 2048, 4096], P('sp', None, 'tp'), may hold values from -0.125 to 0.125
- expert_down: bfloat16 [32, 4096, 2048], P('sp', 'tp'), may hold values from -0.09375 to 0.09375
Outputs:
- layer_out: bfloat16 [8192, 2048], P(('sp', 'tp'))
The draws below stay inside these ranges and needn't reach their ends.
Inputs may be any that keep to these rules, and one draw needn't show every extreme that they name: `routing`: each row names 2 different experts. In each aligned block of 32 rows (the rows of one device) no expert is named by more than 4 rows, a bound that some block reaches.
All inputs are finite; a program needn't handle non-finite values.
Results may differ from the reference program's by a relative error of at most 0.018.
The reference program's roundings to bfloat16 on the way count: a program that leaves them out, or rounds other values in their place, can miss the bound.
Values may be sent and summed in bfloat16 or wider, within the bound.
A program may use at most 128 MiB of HBM per device.

```python
import math
import jax
import jax.numpy as jnp
import numpy as np
from jax import lax

D = 2048
HEAD_WIDTH = 128
QUERY_HEADS = 16
KEY_VALUE_HEADS = 8
FF = 4096
TOP = 2
GRID_W = 64
TOK_DEV = 32
TOKEN_COUNT = 8192
EXPERTS = 32
CAP = 4
N_SP = 32
N_TP = 8


def draw_pair(key):
    base_key = jax.random.fold_in(key, 7)
    query_key, random_key_seed = jax.random.split(base_key, 2)
    query_rows = jax.random.normal(query_key, (TOKEN_COUNT, QUERY_HEADS, HEAD_WIDTH), jnp.float32)
    every_key_row = jax.random.normal(random_key_seed, (TOKEN_COUNT, KEY_VALUE_HEADS, HEAD_WIDTH), jnp.float32)
    query_rows = jnp.clip(query_rows, -6.0, 6.0)
    every_key_row = jnp.clip(every_key_row, -6.0, 6.0)
    return (query_rows.reshape(TOKEN_COUNT, QUERY_HEADS * HEAD_WIDTH), every_key_row.reshape(TOKEN_COUNT, KEY_VALUE_HEADS * HEAD_WIDTH))


def draw_query_proj(key, part):
    return draw_pair(key)[0].astype(jnp.bfloat16)


def draw_projected_key_heads(key, part):
    return draw_pair(key)[1].astype(jnp.bfloat16)


def draw_gains(key, salt):
    values = jax.random.uniform(jax.random.fold_in(key, salt), (HEAD_WIDTH,), jnp.float32)
    return 1.3 + 0.6 * values


def draw_query_gain(key, part):
    return draw_gains(key, 11)


def draw_key_norm_gain(key, part):
    return draw_gains(key, 13)


def block_scale(own_key, extent, cuts, smallest, high):
    level, own = 1.0, jax.random.fold_in(own_key, 6)
    for position, shards_of in cuts:
        steps = jnp.exp(jax.random.uniform(jax.random.fold_in(own, position), (shards_of,), jnp.float32, smallest / len(cuts), high / len(cuts)))
        level = level * jnp.repeat(steps, extent[position] // shards_of).reshape([-1 if axis == position else 1 for axis in range(len(extent))])
    return level


def assign_block(stream_key, own, number, rows, count, top, limit, skew):
    order = jax.random.permutation(stream_key, count)
    packed, common = load_shares(count, rows * top, limit, skew, True), load_shares(count, rows * top, limit, skew, False)
    places = jnp.arange(count)

    def named(sizes, offset_by):
        used = int((sizes > 0).sum())
        fixed = max(1, used // 4)
        shifted = fixed + (places - fixed + offset_by * (used - fixed)) % max(1, count - fixed)
        return jnp.zeros((count,), jnp.int32).at[order[jnp.where(places < fixed, places, shifted)]].set(jnp.asarray(sizes, jnp.int32))

    sizes = jnp.where(number % 4 == 0, named(packed, number // 4), named(common, number - number // 4 - 1))
    mixed = jax.random.permutation(jax.random.fold_in(own, 3), count)
    source_of, receiver = mixed[0:count // 2 * 2:2], mixed[1:count // 2 * 2:2]
    slack = jnp.minimum(sizes[source_of] - 1, limit - sizes[receiver]) // 2
    slack = jnp.where((source_of == order[0]) | (receiver == order[0]) | (sizes[receiver] == 0), 0, jnp.maximum(slack, 0))
    shifted = jax.random.randint(jax.random.fold_in(own, 4), (count // 2,), 0, 1 << 20) % (slack + 1)
    sizes = sizes.at[source_of].add(-shifted).at[receiver].add(shifted)
    items = jnp.searchsorted(jnp.cumsum(sizes), jnp.arange(rows * top), side="right").astype(jnp.int32)
    grid = items.reshape(top, rows).T
    grid = grid[jax.random.permutation(jax.random.fold_in(own, 1), rows)]
    offset_by = jax.random.randint(jax.random.fold_in(own, 2), (rows, 1), 0, top)
    return jnp.take_along_axis(grid, (jnp.arange(top)[None, :] + offset_by) % top, axis=1)


def load_shares(number_of, total, bound, slope, full):
    weights = [(1 << 20) // math.isqrt(rank ** slope) + 1 for rank in range(1, number_of + 1)]
    largest = bound if full else min(bound, max(-(-total // number_of), total * weights[0] // sum(weights)))
    least = 1 if total - largest >= number_of - 1 else 0
    given, rest = [largest] + [least] * (number_of - 1), total - largest - least * (number_of - 1)
    while rest > 0:
        movable = [i for i in range(1, number_of) if given[i] < largest] or [i for i in range(1, number_of) if given[i] < bound]
        whole, left = sum([weights[i] for i in movable]), rest
        for i in movable:
            addition = min(bound - given[i], max(1, left * weights[i] // whole), rest)
            given[i] = given[i] + addition
            rest = rest - addition
    return np.array(given)


def centred(stream_key, extent, scale, bound, shards=(), kind=jnp.bfloat16):
    loudness = block_scale(stream_key, extent, shards, -0.22, 0.18) if shards else 1.0
    drawn = jax.random.normal(stream_key, extent, jnp.float32) * scale * loudness
    return jnp.minimum(jnp.maximum(drawn, -bound), bound).astype(kind)


def setup_inputs(seed: int = 0) -> dict:
    key_of = jax.random.split(jax.random.key(seed), 14)
    x_resid = centred(key_of[0], (TOKEN_COUNT, D), 0.5, 3.0, ((0, 256),))
    query_proj = draw_query_proj(jax.random.fold_in(key_of[13], 71), 0)
    projected_key_heads = draw_projected_key_heads(jax.random.fold_in(key_of[13], 71), 0)
    projected_value_heads = centred(key_of[3], (TOKEN_COUNT, KEY_VALUE_HEADS * HEAD_WIDTH), 1.0, 6.0, ((0, 32), (1, 8)))
    query_gain = draw_query_gain(jax.random.fold_in(key_of[13], 71), 0)
    key_norm_gain = draw_key_norm_gain(jax.random.fold_in(key_of[13], 71), 0)
    out_weight = centred(key_of[6], (QUERY_HEADS * HEAD_WIDTH, D), (QUERY_HEADS * HEAD_WIDTH) ** -0.5, 0.125, ((0, 8),))
    ffn_gain = jnp.clip(1.0 + 0.18 * jax.random.normal(key_of[7], (D,), jnp.float32), 0.1, 1.9)
    routing_keys = jax.random.split(jax.random.fold_in(key_of[8], 1), TOKEN_COUNT // TOK_DEV)
    routing_turns = jax.random.permutation(jax.random.fold_in(key_of[8], 3), TOKEN_COUNT // TOK_DEV)
    routing = jax.vmap(lambda own, number: assign_block(jax.random.fold_in(key_of[8], 2), own, number, TOK_DEV, EXPERTS, TOP, CAP, 2))(routing_keys, routing_turns).reshape((TOKEN_COUNT, TOP))
    route_scores = centred(key_of[9], (TOKEN_COUNT, TOP), 1.5, 6.0, ((0, 256),), jnp.float32)
    expert_gate = centred(key_of[10], (EXPERTS, D, FF), D ** -0.5, 0.125, ((0, 32), (2, 8)))
    expert_up = centred(key_of[11], (EXPERTS, D, FF), D ** -0.5, 0.125, ((0, 32), (2, 8)))
    expert_down = centred(key_of[12], (EXPERTS, FF, D), FF ** -0.5, 0.09375, ((0, 32), (1, 8)))
    return {"x_resid": x_resid, "query_proj": query_proj, "projected_key_heads": projected_key_heads, "projected_value_heads": projected_value_heads, "query_gain": query_gain, "key_norm_gain": key_norm_gain, "out_weight": out_weight, "ffn_gain": ffn_gain, "routing": routing, "route_scores": route_scores, "expert_gate": expert_gate, "expert_up": expert_up, "expert_down": expert_down}


NORM_EPS = 1e-06
ROPE_BASE = 10000.0

def rms_scale(values, norm_gain):
    return values * lax.rsqrt(lax.optimization_barrier(jnp.mean(values * values, axis=-1, keepdims=True)) + NORM_EPS) * norm_gain

def grid_angles(token_positions, head_size):
    freq_count = head_size // 4
    frequency = ROPE_BASE ** (-jnp.arange(freq_count, dtype=jnp.float32) / freq_count)
    grid_row = (token_positions // GRID_W).astype(jnp.float32)
    grid_col = (token_positions % GRID_W).astype(jnp.float32)
    return (grid_row[:, None] * frequency, grid_col[:, None] * frequency)

def turn_half(values, angles):
    cosine = jnp.cos(angles)[:, None, :]
    sine_part = jnp.sin(angles)[:, None, :]
    leading, trailing = jnp.split(values, 2, axis=-1)
    return jnp.concatenate([leading * cosine - trailing * sine_part, trailing * cosine + leading * sine_part], axis=-1)

def normalize_rotate(projected, norm_gain, token_positions, heads):
    length = projected.shape[0]
    values = projected.astype(jnp.float32).reshape(length, heads, -1)
    head_size = values.shape[-1]
    values = rms_scale(values, norm_gain)
    row_angle, col_angle = grid_angles(token_positions, head_size)
    half_size = head_size // 2
    turned = jnp.concatenate([turn_half(values[..., :half_size], row_angle), turn_half(values[..., half_size:], col_angle)], axis=-1)
    return turned.reshape(length, heads * head_size).astype(jnp.bfloat16)

def reference(x_resid, query_proj, projected_key_heads, projected_value_heads, query_gain, key_norm_gain, out_weight, ffn_gain, routing, route_scores, expert_gate, expert_up, expert_down):
    token_positions = jnp.arange(TOKEN_COUNT, dtype=jnp.int32)
    query_rows = normalize_rotate(query_proj, query_gain, token_positions, QUERY_HEADS)
    rotated_key_rows = normalize_rotate(projected_key_heads, key_norm_gain, token_positions, KEY_VALUE_HEADS)
    head_groups = QUERY_HEADS // KEY_VALUE_HEADS
    rows_per_block = math.gcd(TOKEN_COUNT, 256)
    blocks_of_queries = query_rows.reshape(TOKEN_COUNT // rows_per_block, rows_per_block, KEY_VALUE_HEADS, head_groups, HEAD_WIDTH)
    grid_of_keys = rotated_key_rows.reshape(TOKEN_COUNT, KEY_VALUE_HEADS, HEAD_WIDTH).astype(jnp.float32)
    grid_of_values = projected_value_heads.reshape(TOKEN_COUNT, KEY_VALUE_HEADS, HEAD_WIDTH).astype(jnp.float32)

    def attend(query_block):
        scores = jnp.einsum('qhgd,khd->hgqk', query_block.astype(jnp.float32), grid_of_keys) * HEAD_WIDTH ** (-0.5)
        row_top = lax.optimization_barrier(jnp.max(scores, axis=-1, keepdims=True))
        weights = jnp.exp(scores - row_top)
        total = lax.optimization_barrier(jnp.sum(weights, axis=-1))
        rounded = lax.optimization_barrier(weights.astype(jnp.bfloat16)).astype(jnp.float32)
        summed = jnp.einsum('hgqk,khd->qhgd', rounded, grid_of_values)
        return (summed / jnp.transpose(total, (2, 0, 1))[..., None]).astype(jnp.bfloat16)
    attended = lax.map(attend, blocks_of_queries).reshape(TOKEN_COUNT, QUERY_HEADS * HEAD_WIDTH)
    col_width = QUERY_HEADS * HEAD_WIDTH // N_TP
    proj_sum = jnp.zeros((TOKEN_COUNT, D), jnp.float32)
    for block_index in range(N_TP):
        low_col = block_index * col_width
        partial_value = jnp.dot(attended[:, low_col:low_col + col_width], out_weight[low_col:low_col + col_width], preferred_element_type=jnp.float32)
        proj_sum = proj_sum + lax.optimization_barrier(partial_value.astype(jnp.bfloat16)).astype(jnp.float32)
    attn_proj = lax.optimization_barrier(proj_sum.astype(jnp.bfloat16)).astype(jnp.float32)
    middle = x_resid.astype(jnp.float32) + attn_proj
    normed = rms_scale(middle, ffn_gain).astype(jnp.bfloat16)
    flat_expert = routing.reshape(-1).astype(jnp.int32)
    assigned = flat_expert.shape[0]
    flat_token = jnp.arange(assigned, dtype=jnp.int32) // TOP
    flat_gate = jax.nn.softmax(route_scores.astype(jnp.float32), axis=-1).reshape(-1)
    sort_order = jnp.argsort(flat_expert, stable=True)
    sorted_token = flat_token[sort_order]
    sorted_gate = flat_gate[sort_order]
    counts = lax.optimization_barrier(jnp.sum((flat_expert[None, :] == jnp.arange(EXPERTS, dtype=jnp.int32)[:, None]).astype(jnp.int32), axis=1))
    starts = jnp.cumsum(counts) - counts
    most_rows = N_SP * N_TP * CAP
    slot_index = jnp.arange(most_rows, dtype=jnp.int32)
    hidden_width = FF // N_TP

    def run_expert(operands):
        gate_matrix, up_matrix, down_matrix, expert_index = operands
        filled = slot_index < counts[expert_index]
        where_rows = jnp.minimum(starts[expert_index] + slot_index, assigned - 1).astype(jnp.int32)
        token_ids = sorted_token[where_rows]
        inputs = normed[token_ids]
        gate_part = jnp.dot(inputs, gate_matrix, preferred_element_type=jnp.float32)
        up_part = jnp.dot(inputs, up_matrix, preferred_element_type=jnp.float32)
        hidden = (jax.nn.silu(gate_part) * up_part).astype(jnp.bfloat16)
        summed = jnp.zeros((most_rows, D), jnp.float32)
        for block_index in range(N_TP):
            low_row = block_index * hidden_width
            partial_value = jnp.dot(hidden[:, low_row:low_row + hidden_width], down_matrix[low_row:low_row + hidden_width], preferred_element_type=jnp.float32)
            summed = summed + lax.optimization_barrier(partial_value.astype(jnp.bfloat16)).astype(jnp.float32)
        expert_result = lax.optimization_barrier(summed.astype(jnp.bfloat16)).astype(jnp.float32)
        weight = jnp.where(filled, sorted_gate[where_rows], jnp.zeros((most_rows,), jnp.float32))
        targets = jnp.where(filled, token_ids, jnp.full((most_rows,), TOKEN_COUNT, jnp.int32))
        return (expert_result * weight[:, None], targets)
    contrib, targets = lax.map(run_expert, (expert_gate, expert_up, expert_down, jnp.arange(EXPERTS, dtype=jnp.int32)))
    routed = jax.ops.segment_sum(contrib.reshape(-1, D), targets.reshape(-1), num_segments=TOKEN_COUNT + 1)[:TOKEN_COUNT]
    return (middle + routed).astype(jnp.bfloat16)
```

```python
import functools
import jax
import jax.numpy as jnp
from jax import lax
from jax.experimental import pallas as pl
from jax.experimental.pallas import tpu as pltpu
from jax.sharding import PartitionSpec as P

HEAD_WIDTH = 128
TOP = 2
GRID_W = 64
NORM_EPS = 1e-06
ROPE_BASE = 10000.0
NEG_LARGE = -1e30
LOG2E = 1.4426950408889634
MESH = pl.DeviceIdType.MESH

NZ, NX, NY = 8, 4, 4
N_SP = NZ * NX
N_TP = NY * 2
SEQ = 256
ROWS_A = 96
ARRIVALS = [('A', 0, 1), ('A', 0, -1), ('B', 1, 0), ('B', -1, 0), ('B', 0, -1), ('A', 1, 0), ('A', -1, 0), ('A', 0, 2), ('A', 1, 1), ('A', -1, 1), ('B', 0, 1), ('A', 1, -1), ('A', -1, -1), ('B', 1, -1), ('B', 1, 1), ('B', 2, 0), ('B', -2, 0), ('B', -1, -1), ('A', 2, 0), ('A', -2, 0), ('B', -1, 1), ('A', 1, 2), ('A', -1, 2), ('B', 1, 2), ('A', 2, 1), ('A', -2, 1), ('B', 0, 2), ('B', 2, -1), ('A', 2, -1), ('A', -2, -1), ('B', 2, 1), ('B', -2, -1), ('B', 3, 0), ('B', -3, 0), ('B', -2, 1), ('A', 3, 0), ('A', -3, 0), ('B', -1, 2), ('A', 2, 2), ('A', -2, 2), ('B', 2, 2), ('A', 3, 1), ('A', -3, 1), ('B', 3, -1), ('A', 3, -1), ('A', -3, -1), ('B', 3, 1), ('A', -3, 2), ('B', -3, -1), ('B', 4, 0), ('B', -3, 1), ('A', 4, 0), ('A', 4, -1), ('B', 3, 2), ('B', -2, 2), ('A', 3, 2), ('A', 4, 2), ('A', 4, 1), ('B', -3, 2), ('B', 4, 1), ('B', 4, -1), ('B', 4, 2)]


def rms_scale(values, norm_gain):
    return (
        values * lax.rsqrt(jnp.mean(values * values, axis=-1, keepdims=True) + NORM_EPS) * norm_gain
    )


def turn_tables(token_positions):
    freq_count = HEAD_WIDTH // 4
    frequency = ROPE_BASE ** (-jnp.arange(freq_count, dtype=jnp.float32) / freq_count)
    row = (token_positions // GRID_W).astype(jnp.float32)[:, None] * frequency
    col = (token_positions % GRID_W).astype(jnp.float32)[:, None] * frequency
    angles = jnp.concatenate([row, row, col, col], axis=-1)
    sign = jnp.where((jnp.arange(HEAD_WIDTH) // freq_count) % 2 == 0, -1.0, 1.0)
    return jnp.cos(angles), jnp.sin(angles) * sign.astype(jnp.float32)


def turned(values, gain, cos, sin):
    normed = rms_scale(values, gain)
    lane = lax.broadcasted_iota(jnp.int32, normed.shape, 1)
    partner = jnp.where(
        lane % 64 < 32, pltpu.roll(normed, 96, 1), pltpu.roll(normed, 32, 1)
    )
    return (normed * cos + partner * sin).astype(jnp.bfloat16)


def attention_kernel(
    q_ref, k_ref, v_ref, qg_ref, kg_ref, cos_ref, sin_ref, w_ref, x_ref, fg_ref,
    mid_ref, normed_ref,
    kv, qs, m_ref, l_ref, acc, wfull, att, att_in,
    send_sem, recv_a, recv_b, recv_w, recv_att, own_sem,
):
    sp = lax.axis_index("sp")
    tp = lax.axis_index("tp")
    z, x = sp // NX, sp % NX
    y, c = tp // 2, tp % 2

    def sp_of(dz, dx):
        return ((z - dz + 2 * NZ) % NZ) * NX + (x - dx + 2 * NX) % NX

    def tp_of(dy, other=False):
        return ((y + dy + NY) % NY) * 2 + ((1 - c) if other else c)

    own_w = pltpu.make_async_copy(w_ref, wfull.at[tp], own_sem)
    own_w.start()

    barrier = pltpu.get_barrier_semaphore()
    friends = [(sp_of(dz, dx), tp) for dz, dx in ((1, 0), (-1, 0), (0, 1), (0, -1), (0, 2))]
    friends += [(sp, tp_of(dy, o)) for dy in range(NY) for o in (False, True) if (dy, o) != (0, False)]
    for dev in friends:
        pl.semaphore_signal(barrier, inc=1, device_id=dev, device_id_type=MESH)

    cos, sin = cos_ref[...], sin_ref[...]
    kv[sp, :, 0:128] = turned(k_ref[...].astype(jnp.float32), kg_ref[...], cos, sin)
    kv[sp, :, 128:256] = v_ref[...]
    for h in range(2):
        qs[h] = turned(
            q_ref[:, h * 128 : (h + 1) * 128].astype(jnp.float32), qg_ref[...], cos, sin
        )
    m_ref[...] = jnp.full(m_ref.shape, NEG_LARGE, jnp.float32)
    l_ref[...] = jnp.zeros(l_ref.shape, jnp.float32)
    acc[...] = jnp.zeros(acc.shape, jnp.float32)
    pl.semaphore_wait(barrier, len(friends))

    sent = []

    def send(src, dst, recv, dev):
        copy = pltpu.make_async_remote_copy(
            src_ref=src, dst_ref=dst, send_sem=send_sem.at[len(sent)], recv_sem=recv,
            device_id=dev, device_id_type=MESH,
        )
        copy.start()
        sent.append(copy)

    def arrived(ref, recv):
        pltpu.make_async_remote_copy(
            src_ref=ref, dst_ref=ref, send_sem=send_sem.at[0], recv_sem=recv,
            device_id=(sp, tp_of(0, True)), device_id_type=MESH,
        ).wait_recv()

    def piece(half, owner):
        if half == "A":
            return kv.at[owner, pl.ds(0, ROWS_A)], recv_a.at[owner]
        return kv.at[owner, pl.ds(ROWS_A, SEQ - ROWS_A)], recv_b.at[owner]

    def pass_on(half, dz, dx, link):
        ref, recv = piece(half, sp_of(dz, dx))
        dev = {
            "z+": (sp_of(-1, 0), tp), "z-": (sp_of(1, 0), tp),
            "x+": (sp_of(0, -1), tp), "x-": (sp_of(0, 1), tp), "x2": (sp_of(0, 2), tp),
        }[link]
        send(ref, ref, recv, dev)

    def next_links(half, dz, dx):
        if half == "A":
            if dz == 0:
                return ["z+", "z-"]
            if dz in (1, 2) or (dz == 3 and dx in (0, 1)):
                return ["z+"]
            if dz in (-1, -2) or (dz == -3 and dx in (-1, 2)):
                return ["z-"]
            return []
        if dx == 0:
            along = ["z+"] if dz in (1, 2, 3) else ["z-"] if dz in (-1, -2) else []
            return along + ["x+", "x-"]
        if dx == 1 and dz % 2 == 0:
            return ["x+"]
        if dx == -1 and dz % 2 == 1:
            return ["x-"]
        return []

    def w_half(owner, half):
        return wfull.at[owner, pl.ds(half * 128, 128)], recv_w.at[owner, half]

    for half, dz, dx, link in (
        ("B", 0, 0, "z+"), ("B", 0, 0, "z-"), ("A", 0, 0, "x+"), ("A", 0, 0, "x-"),
        ("A", 0, 0, "x2"), ("B", 0, 0, "x+"), ("B", 0, 0, "x-"), ("A", 0, 0, "z+"),
        ("A", 0, 0, "z-"),
    ):
        pass_on(half, dz, dx, link)
    for half, dev in ((0, tp_of(1)), (1, tp_of(-1)), (1, tp_of(1)), (0, tp_of(-1))):
        dst, recv = w_half(tp, half)
        send(w_ref.at[pl.ds(half * 128, 128)], dst, recv, (sp, dev))
    for half in (0, 1):
        dst, recv = w_half(tp, half)
        send(w_ref.at[pl.ds(half * 128, 128)], dst, recv, (sp, tp_of(0, True)))

    def w_event(dy, half, links):
        ref, recv = w_half(tp_of(dy), half)
        arrived(ref, recv)
        for link in links:
            dev = tp_of(0, True) if link == 0 else tp_of(link)
            send(ref, ref, recv, (sp, dev))

    scale2 = HEAD_WIDTH ** (-0.5) * LOG2E

    def attend(group):
        def step(i, carry):
            block = kv[pl.ds(group * NX + 2 * i, 2)].reshape(2 * SEQ, 256)
            keys, values = block[:, 0:128], block[:, 128:256]
            for h in range(2):
                s = lax.dot_general(
                    qs[h], keys, (((1,), (1,)), ((), ())), preferred_element_type=jnp.float32
                )
                m_old = m_ref[h]
                m_new = jnp.maximum(m_old, jnp.max(s, axis=1, keepdims=True))
                alpha = jnp.exp2((m_old - m_new) * scale2)
                m_all = jnp.concatenate([m_new * scale2] * 4, axis=1)
                p = jnp.exp2(s * scale2 - m_all)
                l_ref[h] = l_ref[h] * alpha + (
                    (p[:, 0:128] + p[:, 128:256]) + (p[:, 256:384] + p[:, 384:512])
                )
                acc[h] = acc[h] * alpha + jnp.dot(
                    p.astype(jnp.bfloat16), values, preferred_element_type=jnp.float32
                )
                m_ref[h] = m_new
            return carry

        lax.fori_loop(0, NX // 2, step, 0)

    left = {dz: (6 if dz == 0 else 8) for dz in (0, 1, -1, 2, -2, 3, -3, 4)}
    w_plan = {24: ((-1, 0, (1, 0)), (1, 1, (-1, 0))), 55: ((-1, 1, (0,)), (1, 0, (0,)))}
    ready = []
    for count, (half, dz, dx) in enumerate(ARRIVALS):
        ref, recv = piece(half, sp_of(dz, dx))
        arrived(ref, recv)
        for link in next_links(half, dz, dx):
            pass_on(half, dz, dx, link)
        for dy, w_part, links in w_plan.get(count, ()):
            w_event(dy, w_part, links)
        left[dz] -= 1
        if left[dz] == 0:
            attend((z - dz + NZ) % NZ)

    for h in range(2):
        total = jnp.sum(l_ref[h], axis=1, keepdims=True)
        att[:, h * 128 : (h + 1) * 128] = (acc[h] / total).astype(jnp.bfloat16)

    att_in[tp] = att[pl.ds(tp * 32, 32), :]
    for dy, other in ((0, True), (1, False), (1, True), (3, False), (3, True), (2, False), (2, True)):
        to = tp_of(dy, other)
        send(att.at[pl.ds(to * 32, 32)], att_in.at[tp], recv_att.at[tp], (sp, to))

    own_w.wait()
    w_event(2, 0, (0,))
    w_event(2, 1, (0,))
    total = jnp.zeros((32, 2048), jnp.float32)
    order = [(0, False), (0, True), (1, False), (3, False), (1, True), (3, True), (2, False), (2, True)]
    for dy, other in order:
        owner = tp_of(dy, other)
        if (dy, other) != (0, False):
            arrived(att_in.at[owner], recv_att.at[owner])
        if other:
            for half in (0, 1):
                ref, recv = w_half(owner, half)
                arrived(ref, recv)
        part = jnp.dot(att_in[owner], wfull[owner], preferred_element_type=jnp.float32)
        total = total + part.astype(jnp.bfloat16).astype(jnp.float32)
    middle = x_ref[...].astype(jnp.float32) + total.astype(jnp.bfloat16).astype(jnp.float32)
    mid_ref[...] = middle
    normed_ref[...] = rms_scale(middle, fg_ref[...]).astype(jnp.bfloat16)
    for copy in sent:
        copy.wait_send()


def attention_part(x_resid, query_proj, keys, values, query_gain, key_gain, out_weight, ffn_gain):
    positions = lax.axis_index("sp") * SEQ + jnp.arange(SEQ, dtype=jnp.int32)
    cos, sin = turn_tables(positions)
    vmem = pl.BlockSpec(memory_space=pltpu.VMEM)
    return pl.pallas_call(
        attention_kernel,
        out_shape=(
            jax.ShapeDtypeStruct((32, 2048), jnp.float32),
            jax.ShapeDtypeStruct((32, 2048), jnp.bfloat16),
        ),
        in_specs=[vmem] * 7 + [pl.BlockSpec(memory_space=pl.ANY)] + [vmem] * 2,
        out_specs=(vmem, vmem),
        scratch_shapes=[
            pltpu.VMEM((N_SP, SEQ, 256), jnp.bfloat16),
            pltpu.VMEM((2, SEQ, 128), jnp.bfloat16),
            pltpu.VMEM((2, SEQ, 128), jnp.float32),
            pltpu.VMEM((2, SEQ, 128), jnp.float32),
            pltpu.VMEM((2, SEQ, 128), jnp.float32),
            pltpu.VMEM((N_TP, 256, 2048), jnp.bfloat16),
            pltpu.VMEM((SEQ, 256), jnp.bfloat16),
            pltpu.VMEM((N_TP, 32, 256), jnp.bfloat16),
            pltpu.SemaphoreType.DMA((96,)),
            pltpu.SemaphoreType.DMA((N_SP,)),
            pltpu.SemaphoreType.DMA((N_SP,)),
            pltpu.SemaphoreType.DMA((N_TP, 2)),
            pltpu.SemaphoreType.DMA((N_TP,)),
            pltpu.SemaphoreType.DMA,
        ],
        compiler_params=pltpu.CompilerParams(
            collective_id=0, has_side_effects=True, vmem_limit_bytes=40 * 1024 * 1024
        ),
        name="attention",
    )(
        query_proj, keys, values, query_gain.reshape(1, -1), key_gain.reshape(1, -1), cos, sin,
        out_weight, x_resid, ffn_gain.reshape(1, -1),
    )


def local(
    x_resid,
    query_proj,
    projected_key_heads,
    projected_value_heads,
    query_gain,
    key_norm_gain,
    out_weight,
    ffn_gain,
    routing,
    route_scores,
    expert_gate,
    expert_up,
    expert_down,
):
    own_tokens = x_resid.shape[0]
    model_width = x_resid.shape[1]
    middle, normed = attention_part(
        x_resid, query_proj, projected_key_heads, projected_value_heads, query_gain,
        key_norm_gain, out_weight, ffn_gain,
    )
    experts_all = lax.axis_size("sp") * expert_gate.shape[0]
    capacity = max(2, 2 * own_tokens * TOP // experts_all)
    flat_expert = routing.reshape(-1)
    one_hot = (flat_expert[:, None] == jnp.arange(experts_all, dtype=jnp.int32)[None, :]).astype(
        jnp.int32
    )
    earlier = jnp.cumsum(one_hot, axis=0) - one_hot
    slot_rank = jnp.sum(earlier * one_hot, axis=1)
    target = flat_expert * capacity + slot_rank
    chooser = (
        jnp.arange(experts_all * capacity, dtype=jnp.int32)[:, None] == target[None, :]
    ).astype(jnp.float32)
    gate_share = jax.nn.softmax(route_scores, axis=-1).reshape(-1)
    picker = jnp.sum(chooser.reshape(experts_all * capacity, own_tokens, TOP), axis=2).astype(
        jnp.bfloat16
    )
    combiner = jnp.sum(
        (chooser * gate_share[None, :]).reshape(experts_all * capacity, own_tokens, TOP), axis=2
    )
    dispatch = (
        jnp.dot(picker, normed, preferred_element_type=jnp.float32)
        .astype(jnp.bfloat16)
        .reshape(experts_all, capacity, model_width)
    )
    gate_matrix = expert_gate[0]
    up_matrix = expert_up[0]
    down_matrix = expert_down[0]
    arrived = lax.all_to_all(dispatch, "sp", split_axis=0, concat_axis=0, tiled=True)
    row_block = lax.all_gather(arrived.reshape(-1, model_width), "tp", axis=0, tiled=True)
    gate_part = jnp.dot(row_block, gate_matrix, preferred_element_type=jnp.float32)
    up_part = jnp.dot(row_block, up_matrix, preferred_element_type=jnp.float32)
    hidden = (jax.nn.silu(gate_part) * up_part).astype(jnp.bfloat16)
    row_block = hidden
    expert_result = lax.psum_scatter(
        jnp.dot(row_block, down_matrix, preferred_element_type=jnp.float32).astype(jnp.bfloat16),
        "tp",
        scatter_dimension=0,
        tiled=True,
    )
    returned = lax.all_to_all(
        expert_result.reshape(-1, capacity, model_width),
        "sp",
        split_axis=0,
        concat_axis=0,
        tiled=True,
    )
    routed = jnp.einsum(
        "st,sd->td", combiner, returned.reshape(-1, model_width).astype(jnp.float32)
    )
    return (middle + routed).astype(jnp.bfloat16)


def solution(mesh):
    in_specs = (
        P(("sp", "tp"), None),
        P("sp", "tp"),
        P("sp", "tp"),
        P("sp", "tp"),
        P(),
        P(),
        P("tp", None),
        P(),
        P(("sp", "tp"), None),
        P(("sp", "tp"), None),
        P("sp", None, "tp"),
        P("sp", None, "tp"),
        P("sp", "tp", None),
    )
    out_specs = P(("sp", "tp"), None)
    return jax.shard_map(local, mesh=mesh, in_specs=in_specs, out_specs=out_specs, check_vma=False)
```

```python
import functools
import jax
import jax.numpy as jnp
import numpy as np
from jax import lax
from jax.experimental import pallas as pl
from jax.experimental.pallas import tpu as pltpu
from jax.sharding import PartitionSpec as P

HEAD_WIDTH = 128
TOP = 2
GRID_W = 64
NORM_EPS = 1e-06
ROPE_BASE = 10000.0
NEG_LARGE = -1e30
LOG2E = 1.4426950408889634
MESH = pl.DeviceIdType.MESH

NZ, NX, NY = 8, 4, 4
N_SP = NZ * NX
N_TP = NY * 2
SEQ = 256
ROWS_A = 96
ARRIVALS = [('A', 0, 1), ('A', 0, -1), ('B', 1, 0), ('B', -1, 0), ('B', 0, -1), ('A', 1, 0), ('A', -1, 0), ('A', 0, 2), ('A', 1, 1), ('A', -1, 1), ('B', 0, 1), ('A', 1, -1), ('A', -1, -1), ('B', 1, -1), ('B', 1, 1), ('B', 2, 0), ('B', -2, 0), ('B', -1, -1), ('A', 2, 0), ('A', -2, 0), ('B', -1, 1), ('A', 1, 2), ('A', -1, 2), ('B', 1, 2), ('A', 2, 1), ('A', -2, 1), ('B', 0, 2), ('B', 2, -1), ('A', 2, -1), ('A', -2, -1), ('B', 2, 1), ('B', -2, -1), ('B', 3, 0), ('B', -3, 0), ('B', -2, 1), ('A', 3, 0), ('A', -3, 0), ('B', -1, 2), ('A', 2, 2), ('A', -2, 2), ('B', 2, 2), ('A', 3, 1), ('A', -3, 1), ('B', 3, -1), ('A', 3, -1), ('A', -3, -1), ('B', 3, 1), ('A', -3, 2), ('B', -3, -1), ('B', 4, 0), ('B', -3, 1), ('A', 4, 0), ('A', 4, -1), ('B', 3, 2), ('B', -2, 2), ('A', 3, 2), ('A', 4, 2), ('A', 4, 1), ('B', -3, 2), ('B', 4, 1), ('B', 4, -1), ('B', 4, 2)]


def rms_scale(values, norm_gain):
    return (
        values * lax.rsqrt(jnp.mean(values * values, axis=-1, keepdims=True) + NORM_EPS) * norm_gain
    )


EXPERTS, CAP = 32, 4
BACK = (0, 1, -1, 2, -2, 3, -3, 4)


def turn_tables():
    freq_count = HEAD_WIDTH // 4
    frequency = np.power(ROPE_BASE, -np.arange(freq_count) / freq_count).astype(np.float32)
    place = np.arange(N_SP * SEQ // GRID_W, dtype=np.float32)
    angles = np.tile(place[:, None] * frequency, (1, 4)).astype(np.float64)
    sign = np.where((np.arange(HEAD_WIDTH) // freq_count) % 2 == 0, -1.0, 1.0)
    return jnp.asarray(np.stack([np.cos(angles), np.sin(angles) * sign]).astype(np.float32))


def turned(values, gain, cos, sin):
    normed = rms_scale(values, gain)
    lane = lax.broadcasted_iota(jnp.int32, normed.shape, 1)
    partner = jnp.where(
        lane % 64 < 32, pltpu.roll(normed, 96, 1), pltpu.roll(normed, 32, 1)
    )
    return (normed * cos + partner * sin).astype(jnp.bfloat16)


def iota(shape, dim):
    return lax.broadcasted_iota(jnp.int32, shape, dim)


def layer_kernel(
    q_hbm, k_hbm, v_hbm, gains_hbm, table_hbm, w_hbm, x_hbm, fg_hbm, routing_hbm, scores_hbm,
    gate_hbm, up_hbm, down_hbm,
    out_ref,
    q_ref, k_ref, gains_ref, table_ref, x_ref, fg_ref, routing_ref, scores_ref,
    wg, wu, wd,
    kv, qs, m_ref, l_ref, acc, wfull, att, att_in,
    slots, rows_in, xr, parts, parts_in, near_out, far_in, near_in, back, returned, middle_ref,
    send_sem, recv_a, recv_b, recv_w, recv_att, load_sem,
    recv_x, recv_part, recv_far, recv_near, recv_back,
):
    sp = lax.axis_index("sp")
    tp = lax.axis_index("tp")
    z, x = sp // NX, sp % NX
    y, c = tp // 2, tp % 2

    def sp_of(dz, dx):
        return ((z - dz + 2 * NZ) % NZ) * NX + (x - dx + 2 * NX) % NX

    def tp_of(dy, other=False):
        return ((y + dy + NY) % NY) * 2 + ((1 - c) if other else c)

    loads = {}
    for n, (name, src, dst) in enumerate((
        ("k", k_hbm, k_ref), ("v", v_hbm, kv.at[sp, :, pl.ds(128, 128)]), ("gains", gains_hbm, gains_ref),
        ("table", table_hbm, table_ref), ("q", q_hbm, q_ref),
        ("w", w_hbm, wfull.at[tp]), ("x", x_hbm, x_ref), ("fg", fg_hbm, fg_ref),
        ("routing", routing_hbm, routing_ref), ("scores", scores_hbm, scores_ref),
        ("gate", gate_hbm.at[0], wg), ("up", up_hbm.at[0], wu), ("down", down_hbm.at[0], wd),
    )):
        loads[name] = pltpu.make_async_copy(src, dst, load_sem.at[n])
        loads[name].start()

    barrier = pltpu.get_barrier_semaphore()

    def greet(i, carry):
        pl.semaphore_signal(barrier, inc=1, device_id=((sp + i) % N_SP, tp), device_id_type=MESH)
        return carry

    lax.fori_loop(1, N_SP, greet, 0)

    def greet_tp(i, carry):
        pl.semaphore_signal(barrier, inc=1, device_id=(sp, (tp + i) % N_TP), device_id_type=MESH)
        return carry

    lax.fori_loop(1, N_TP, greet_tp, 0)

    for name in ("k", "v", "gains", "table"):
        loads[name].wait()

    def table(which):
        lane = iota((GRID_W, 128), 1)
        cols = table_ref[which, 0:GRID_W, :]
        return jnp.concatenate(
            [
                jnp.where(lane < 64, table_ref[which, pl.ds(sp * (SEQ // GRID_W) + i, 1), :], cols)
                for i in range(SEQ // GRID_W)
            ],
            axis=0,
        )

    cos, sin = table(0), table(1)
    kv[sp, :, 0:128] = turned(k_ref[...].astype(jnp.float32), gains_ref[1:2, :], cos, sin)
    loads["q"].wait()
    for h in range(2):
        qs[h] = turned(
            q_ref[:, h * 128 : (h + 1) * 128].astype(jnp.float32), gains_ref[0:1, :], cos, sin
        )
    m_ref[...] = jnp.full(m_ref.shape, NEG_LARGE, jnp.float32)
    l_ref[...] = jnp.zeros(l_ref.shape, jnp.float32)
    acc[...] = jnp.zeros(acc.shape, jnp.float32)
    pl.semaphore_wait(barrier, N_SP + N_TP - 2)

    sent = []

    def send(src, dst, recv, dev):
        copy = pltpu.make_async_remote_copy(
            src_ref=src, dst_ref=dst, send_sem=send_sem.at[len(sent)], recv_sem=recv,
            device_id=dev, device_id_type=MESH,
        )
        copy.start()
        sent.append(copy)

    def arrived(ref, recv):
        pltpu.make_async_remote_copy(
            src_ref=ref, dst_ref=ref, send_sem=send_sem.at[0], recv_sem=recv,
            device_id=(sp, tp_of(0, True)), device_id_type=MESH,
        ).wait_recv()

    def piece(half, owner):
        if half == "A":
            return kv.at[owner, pl.ds(0, ROWS_A)], recv_a.at[owner]
        return kv.at[owner, pl.ds(ROWS_A, SEQ - ROWS_A)], recv_b.at[owner]

    def pass_on(half, dz, dx, link):
        ref, recv = piece(half, sp_of(dz, dx))
        dev = {
            "z+": (sp_of(-1, 0), tp), "z-": (sp_of(1, 0), tp),
            "x+": (sp_of(0, -1), tp), "x-": (sp_of(0, 1), tp), "x2": (sp_of(0, 2), tp),
        }[link]
        send(ref, ref, recv, dev)

    def next_links(half, dz, dx):
        if half == "A":
            if dz == 0:
                return ["z+", "z-"]
            if dz in (1, 2) or (dz == 3 and dx in (0, 1)):
                return ["z+"]
            if dz in (-1, -2) or (dz == -3 and dx in (-1, 2)):
                return ["z-"]
            return []
        if dx == 0:
            along = ["z+"] if dz in (1, 2, 3) else ["z-"] if dz in (-1, -2) else []
            return along + ["x+", "x-"]
        if dx == 1 and dz % 2 == 0:
            return ["x+"]
        if dx == -1 and dz % 2 == 1:
            return ["x-"]
        return []

    def w_half(owner, half):
        return wfull.at[owner, pl.ds(half * 128, 128)], recv_w.at[owner, half]

    for half, dz, dx, link in (
        ("B", 0, 0, "z+"), ("B", 0, 0, "z-"), ("A", 0, 0, "x+"), ("A", 0, 0, "x-"),
        ("A", 0, 0, "x2"), ("B", 0, 0, "x+"), ("B", 0, 0, "x-"), ("A", 0, 0, "z+"),
        ("A", 0, 0, "z-"),
    ):
        pass_on(half, dz, dx, link)
    for half, dev in ((0, tp_of(1)), (1, tp_of(-1)), (1, tp_of(1)), (0, tp_of(-1))):
        dst, recv = w_half(tp, half)
        send(w_hbm.at[pl.ds(half * 128, 128)], dst, recv, (sp, dev))
    for half in (0, 1):
        dst, recv = w_half(tp, half)
        send(w_hbm.at[pl.ds(half * 128, 128)], dst, recv, (sp, tp_of(0, True)))

    def w_event(dy, half, links):
        ref, recv = w_half(tp_of(dy), half)
        arrived(ref, recv)
        for link in links:
            dev = tp_of(0, True) if link == 0 else tp_of(link)
            send(ref, ref, recv, (sp, dev))

    scale2 = HEAD_WIDTH ** (-0.5) * LOG2E

    def attend(group):
        def step(i, carry):
            block = kv[pl.ds(group * NX + 2 * i, 2)].reshape(2 * SEQ, 256)
            keys, values = block[:, 0:128], block[:, 128:256]
            for h in range(2):
                s = lax.dot_general(
                    qs[h], keys, (((1,), (1,)), ((), ())), preferred_element_type=jnp.float32
                )
                m_old = m_ref[h]
                m_new = jnp.maximum(m_old, jnp.max(s, axis=1, keepdims=True))
                alpha = jnp.exp2((m_old - m_new) * scale2)
                m_all = jnp.concatenate([m_new * scale2] * 4, axis=1)
                p = jnp.exp2(s * scale2 - m_all)
                l_ref[h] = l_ref[h] * alpha + (
                    (p[:, 0:128] + p[:, 128:256]) + (p[:, 256:384] + p[:, 384:512])
                )
                acc[h] = acc[h] * alpha + jnp.dot(
                    p.astype(jnp.bfloat16), values, preferred_element_type=jnp.float32
                )
                m_ref[h] = m_new
            return carry

        lax.fori_loop(0, NX // 2, step, 0)

    left = {dz: (6 if dz == 0 else 8) for dz in (0, 1, -1, 2, -2, 3, -3, 4)}
    w_plan = {24: ((-1, 0, (1, 0)), (1, 1, (-1, 0))), 55: ((-1, 1, (0,)), (1, 0, (0,)))}
    for count, (half, dz, dx) in enumerate(ARRIVALS):
        ref, recv = piece(half, sp_of(dz, dx))
        arrived(ref, recv)
        for link in next_links(half, dz, dx):
            pass_on(half, dz, dx, link)
        for dy, w_part, links in w_plan.get(count, ()):
            w_event(dy, w_part, links)
        left[dz] -= 1
        if left[dz] == 0:
            attend((z - dz + NZ) % NZ)

    for h in range(2):
        total = jnp.sum(l_ref[h], axis=1, keepdims=True)
        att[:, h * 128 : (h + 1) * 128] = (acc[h] / total).astype(jnp.bfloat16)

    att_in[tp] = att[pl.ds(tp * 32, 32), :]
    for dy, other in ((0, True), (1, False), (1, True), (3, False), (3, True), (2, False), (2, True)):
        to = tp_of(dy, other)
        send(att.at[pl.ds(to * 32, 32)], att_in.at[tp], recv_att.at[tp], (sp, to))

    for name in ("routing", "scores"):
        loads[name].wait()
    expert_no = iota((32, EXPERTS), 1)
    first = (routing_ref[:, 0:1] == expert_no).astype(jnp.float32)
    second = (routing_ref[:, 1:2] == expert_no).astype(jnp.float32)
    top = jnp.maximum(scores_ref[:, 0:1], scores_ref[:, 1:2])
    e0, e1 = jnp.exp(scores_ref[:, 0:1] - top), jnp.exp(scores_ref[:, 1:2] - top)
    gates = first * (e0 / (e0 + e1)) + second * (e1 / (e0 + e1))
    named = first + second
    before = (iota((32, 32), 1) < iota((32, 32), 0)).astype(jnp.bfloat16)
    rank = jnp.dot(before, named.astype(jnp.bfloat16), preferred_element_type=jnp.float32)
    slot = jnp.where(named > 0.5, rank, -1.0)
    slot4 = jnp.concatenate([slot] * 4, axis=0).astype(jnp.bfloat16)
    gates4 = jnp.concatenate([gates] * 4, axis=0)
    spread = (iota((512, EXPERTS), 0) // 16 == iota((512, EXPERTS), 1)).astype(jnp.bfloat16)
    contract = (((1,), (1,)), ((), ()))
    slot_rows = lax.dot_general(spread, slot4, contract, preferred_element_type=jnp.float32)
    row = iota((512, 128), 0)
    pick = (
        (slot_rows == (row % 4).astype(jnp.float32)) & ((row // 4) % 4 == iota((512, 128), 1) // 32)
    ).astype(jnp.bfloat16)
    slot_cols = lax.dot_general(slot4, spread, contract, preferred_element_type=jnp.float32)
    gate_cols = lax.dot_general(
        gates4, spread.astype(jnp.float32), contract, preferred_element_type=jnp.float32,
        precision=lax.Precision.HIGHEST,
    )
    col = iota((128, 512), 1)
    merge = jnp.where(
        (slot_cols == (col % 4).astype(jnp.float32)) & ((col // 4) % 4 == iota((128, 512), 0) // 32),
        gate_cols, 0.0,
    )

    for name in ("w", "x", "fg"):
        loads[name].wait()
    w_event(2, 0, (0,))
    w_event(2, 1, (0,))
    total = jnp.zeros((32, 2048), jnp.float32)
    order = [(0, False), (0, True), (1, False), (3, False), (1, True), (3, True), (2, False), (2, True)]
    for dy, other in order:
        owner = tp_of(dy, other)
        if (dy, other) != (0, False):
            arrived(att_in.at[owner], recv_att.at[owner])
        if other:
            for half in (0, 1):
                ref, recv = w_half(owner, half)
                arrived(ref, recv)
        part = jnp.dot(att_in[owner], wfull[owner], preferred_element_type=jnp.float32)
        total = total + part.astype(jnp.bfloat16).astype(jnp.float32)
    middle = x_ref[...].astype(jnp.float32) + total.astype(jnp.bfloat16).astype(jnp.float32)
    middle_ref[...] = middle
    normed = rms_scale(middle, fg_ref[...]).astype(jnp.bfloat16)

    stacked = jnp.concatenate([normed[:, 512 * j : 512 * (j + 1)] for j in range(4)], axis=0)
    slots[...] = (
        jnp.dot(pick, stacked, preferred_element_type=jnp.float32)
        .astype(jnp.bfloat16)
        .reshape(EXPERTS, 16, 512)
    )
    rows_in[tp, 0, x] = slots[sp]
    for g, dz in enumerate(BACK):
        for dx in (0, 1, -1, 2):
            if (dz, dx) != (0, 0):
                to = sp_of(-dz, -dx)
                send(slots.at[to], rows_in.at[tp, g, x], recv_x.at[tp, g], (to, tp))

    out_no, in_no = iota((128, 128), 0), iota((128, 128), 1)
    sort = (
        in_no == (out_no % 32 // 4) * 16 + (out_no // 32) * 4 + out_no % 4
    ).astype(jnp.bfloat16)
    out_no, in_no = in_no, out_no
    unsort = (
        in_no == (out_no % 32 // 4) * 16 + (out_no // 32) * 4 + out_no % 4
    ).astype(jnp.bfloat16)

    def group_of(owner, g):
        return rows_in.at[owner, g], recv_x.at[owner, g]

    def spread_rows(owner, g, links):
        ref, recv = group_of(owner, g)
        for link in links:
            dev = tp_of(0, True) if link == 0 else tp_of(link)
            send(ref, ref, recv, (sp, dev))

    def own(g):
        ref, recv = group_of(tp, g)
        arrived(rows_in.at[tp, g, pl.ds(0, 3)] if g == 0 else ref, recv)
        spread_rows(tp, g, (1, -1, 0))

    def near(g):
        for dy in (-1, 1):
            owner = tp_of(dy)
            arrived(*group_of(owner, g))
            spread_rows(owner, g, ((-dy, 0) if (g % 2 == 0) == (dy == -1) else (0,)))

    def far(g):
        owner = tp_of(2)
        arrived(*group_of(owner, g))
        spread_rows(owner, g, (0,))

    def other(g):
        for dy in (0, -1, 1, 2):
            arrived(*group_of(tp_of(dy, True), g))

    def experts(o):
        def sorted_rows(t, carry):
            block = rows_in[t, pl.ds(2 * o, 2)].reshape(128, 512)
            out = jnp.dot(sort, block, preferred_element_type=jnp.float32).astype(jnp.bfloat16)
            at = pl.ds(pl.multiple_of(t * 32, 32), 32)
            for j in range(4):
                xr[at, 512 * j : 512 * (j + 1)] = out[32 * j : 32 * (j + 1)]
            return carry

        lax.fori_loop(0, N_TP, sorted_rows, 0)
        rows = xr[...]
        gate_part = jnp.dot(rows, wg[...], preferred_element_type=jnp.float32)
        up_part = jnp.dot(rows, wu[...], preferred_element_type=jnp.float32)
        hidden = (gate_part / (1.0 + jnp.exp(-gate_part)) * up_part).astype(jnp.bfloat16)
        for j in range(4):
            cols = slice(512 * j, 512 * (j + 1))
            part = jnp.dot(hidden, wd[:, cols], preferred_element_type=jnp.float32)
            parts[o, :, :, cols] = part.astype(jnp.bfloat16).reshape(N_TP, 32, 512)
        for dy in (2, 1, -1, 0):
            home = (y + dy + NY) % NY
            send(
                parts.at[o, tp_of(dy, True)], parts_in.at[o, home], recv_part.at[o, home],
                (sp, tp_of(0, True)),
            )

    def chip_sum(o, dy):
        home = (y + dy + NY) % NY
        arrived(parts_in.at[o, home], recv_part.at[o, home])
        return parts[o, tp_of(dy)].astype(jnp.float32) + parts_in[o, home].astype(jnp.float32)

    def reduce_far(o):
        near_out[o, 0] = chip_sum(o, 2).astype(jnp.bfloat16)
        send(near_out.at[o, 0, pl.ds(0, 16)], far_in.at[o, 0], recv_far.at[o, 0], (sp, tp_of(1)))
        send(near_out.at[o, 0, pl.ds(16, 16)], far_in.at[o, 1], recv_far.at[o, 1], (sp, tp_of(-1)))

    def reduce_near(o):
        for n, dy in ((0, 1), (1, -1)):
            mine = chip_sum(o, dy)
            arrived(far_in.at[o, n], recv_far.at[o, n])
            at = slice(16 * n, 16 * n + 16)
            rest = slice(16 - 16 * n, 32 - 16 * n)
            near_out[o, 1 + n, at, :] = (
                mine[at] + far_in[o, n].astype(jnp.float32)
            ).astype(jnp.bfloat16)
            near_out[o, 1 + n, rest, :] = mine[rest].astype(jnp.bfloat16)
        for n, dy in ((0, 1), (1, -1)):
            send(near_out.at[o, 1 + n], near_in.at[o, n], recv_near.at[o, n], (sp, tp_of(dy)))

    def give_back(o):
        whole = chip_sum(o, 0)
        for n in (0, 1):
            arrived(near_in.at[o, n], recv_near.at[o, n])
            whole = whole + near_in[o, n].astype(jnp.float32)
        result = whole.astype(jnp.bfloat16)
        stack = jnp.concatenate([result[:, 512 * j : 512 * (j + 1)] for j in range(4)], axis=0)
        back[o] = (
            jnp.dot(unsort, stack, preferred_element_type=jnp.float32)
            .astype(jnp.bfloat16)
            .reshape(8, 16, 512)
        )
        if o == 0:
            returned[sp] = back[0, x]
        for n in (0, 1):
            dz = BACK[2 * o + n]
            for dx in (0, 1, -1, 2):
                if (dz, dx) != (0, 0):
                    to = sp_of(dz, dx)
                    send(back.at[o, 4 * n + to % NX], returned.at[sp], recv_back, (to, tp))

    own(0); own(1); own(2); near(0); own(3); near(1); far(0); own(4); near(2); far(1)
    other(0); other(1)
    for name in ("gate", "up", "down"):
        loads[name].wait()
    experts(0)
    own(5); near(3); far(2); reduce_far(0); own(6); near(4); far(3); other(2); other(3)
    experts(1)
    reduce_near(0); own(7); near(5); far(4); reduce_far(1); near(6); far(5); other(4); other(5)
    experts(2)
    give_back(0); reduce_near(1); near(7); far(6); reduce_far(2); far(7); other(6); other(7)
    experts(3)
    give_back(1); reduce_near(2); reduce_far(3); give_back(2); reduce_near(3); give_back(3)

    arrived(returned.at[pl.ds(0, N_SP - 1)], recv_back)
    results = returned[...].reshape(512, 512)
    routed = jnp.dot(
        merge, results.astype(jnp.float32), preferred_element_type=jnp.float32,
        precision=lax.Precision.HIGHEST,
    )
    for j in range(4):
        cols = slice(512 * j, 512 * (j + 1))
        out_ref[:, cols] = (middle_ref[:, cols] + routed[32 * j : 32 * (j + 1)]).astype(jnp.bfloat16)
    for copy in sent:
        copy.wait_send()


def local(
    x_resid,
    query_proj,
    projected_key_heads,
    projected_value_heads,
    query_gain,
    key_norm_gain,
    out_weight,
    ffn_gain,
    routing,
    route_scores,
    expert_gate,
    expert_up,
    expert_down,
):
    hbm = pl.BlockSpec(memory_space=pltpu.HBM)
    bf16, f32 = jnp.bfloat16, jnp.float32
    dma = pltpu.SemaphoreType.DMA
    return pl.pallas_call(
        layer_kernel,
        out_shape=jax.ShapeDtypeStruct((32, 2048), bf16),
        in_specs=[hbm] * 13,
        out_specs=pl.BlockSpec(memory_space=pltpu.VMEM),
        scratch_shapes=[
            pltpu.VMEM((SEQ, 256), bf16),
            pltpu.VMEM((SEQ, 128), bf16),
            pltpu.VMEM((2, 128), f32),
            pltpu.VMEM((2, 128, 128), f32),
            pltpu.VMEM((32, 2048), bf16),
            pltpu.VMEM((1, 2048), f32),
            pltpu.VMEM((32, 2), jnp.int32),
            pltpu.VMEM((32, 2), f32),
            pltpu.VMEM((2048, 512), bf16),
            pltpu.VMEM((2048, 512), bf16),
            pltpu.VMEM((512, 2048), bf16),
            pltpu.VMEM((N_SP, SEQ, 256), bf16),
            pltpu.VMEM((2, SEQ, 128), bf16),
            pltpu.VMEM((2, SEQ, 128), f32),
            pltpu.VMEM((2, SEQ, 128), f32),
            pltpu.VMEM((2, SEQ, 128), f32),
            pltpu.VMEM((N_TP, 256, 2048), bf16),
            pltpu.VMEM((SEQ, 256), bf16),
            pltpu.VMEM((N_TP, 32, 256), bf16),
            pltpu.VMEM((EXPERTS, 16, 512), bf16),
            pltpu.VMEM((N_TP, 8, NX, 16, 512), bf16),
            pltpu.VMEM((256, 2048), bf16),
            pltpu.VMEM((4, N_TP, 32, 2048), bf16),
            pltpu.VMEM((4, NY, 32, 2048), bf16),
            pltpu.VMEM((4, 3, 32, 2048), bf16),
            pltpu.VMEM((4, 2, 16, 2048), bf16),
            pltpu.VMEM((4, 2, 32, 2048), bf16),
            pltpu.VMEM((4, 8, 16, 512), bf16),
            pltpu.VMEM((EXPERTS, 16, 512), bf16),
            pltpu.VMEM((32, 2048), f32),
            dma((256,)),
            dma((N_SP,)),
            dma((N_SP,)),
            dma((N_TP, 2)),
            dma((N_TP,)),
            dma((13,)),
            dma((N_TP, 8)),
            dma((4, NY)),
            dma((4, 2)),
            dma((4, 2)),
            dma,
        ],
        compiler_params=pltpu.CompilerParams(
            collective_id=0, has_side_effects=True, vmem_limit_bytes=60 * 1024 * 1024
        ),
        name="layer",
    )(
        query_proj, projected_key_heads, projected_value_heads,
        jnp.stack([query_gain, key_norm_gain]), turn_tables(), out_weight, x_resid,
        ffn_gain.reshape(1, -1), routing, route_scores, expert_gate, expert_up, expert_down,
    )


def solution(mesh):
    in_specs = (
        P(("sp", "tp"), None),
        P("sp", "tp"),
        P("sp", "tp"),
        P("sp", "tp"),
        P(),
        P(),
        P("tp", None),
        P(),
        P(("sp", "tp"), None),
        P(("sp", "tp"), None),
        P("sp", None, "tp"),
        P("sp", None, "tp"),
        P("sp", "tp", None),
    )
    out_specs = P(("sp", "tp"), None)
    return jax.shard_map(local, mesh=mesh, in_specs=in_specs, out_specs=out_specs, check_vma=False)
```

```python
import functools
import jax
import jax.numpy as jnp
import numpy as np
from jax import lax
from jax.experimental import pallas as pl
from jax.experimental.pallas import tpu as pltpu
from jax.sharding import PartitionSpec as P

HEAD_WIDTH = 128
TOP = 2
GRID_W = 64
NORM_EPS = 1e-06
ROPE_BASE = 10000.0
NEG_LARGE = -1e30
LOG2E = 1.4426950408889634
MESH = pl.DeviceIdType.MESH

NZ, NX, NY = 8, 4, 4
N_SP = NZ * NX
N_TP = NY * 2
SEQ = 256
ROWS_A = 96
ATTENTION_STEPS = (('A', 0, -1), ('A', 0, 1), ('B', -1, 0), ('B', 1, 0), ('A', 0, 2), ('A', -1, 0), ('A', 1, 0),
    ('B', 0, -1), ('A', -1, -1), ('A', 1, -1), ('B', 0, 1), ('A', -1, 1), ('A', 1, 1), ('B', -1, -1),
    ('B', -1, 1), ('B', -2, 0), ('B', 2, 0), ('B', 1, -1), ('A', -1, 2), ('A', 1, 2), ('B', 1, 1),
    ('A', -2, 0), ('A', 2, 0), ('B', -1, 2), ('C', -1, 0), ('A', -2, -1), ('A', 2, -1), ('B', 0, 2),
    ('C', -1, 1), ('A', -2, 1), ('A', 2, 1), ('B', -2, -1), ('C', 0, 0), ('B', -2, 1), ('C', 0, 1),
    ('B', -3, 0), ('B', 3, 0), ('B', 2, -1), ('B', 2, 1), ('A', -2, 2), ('A', 2, 2), ('B', 1, 2),
    ('C', 1, 0), ('A', 3, 0), ('A', -3, 0), ('C', 1, 1), ('A', -3, -1), ('A', 3, -1), ('B', -2, 2),
    ('C', -2, 0), ('A', 3, 1), ('B', -3, -1), ('A', -3, 1), ('C', -2, 1), ('A', -3, 2), ('B', -3, 1),
    ('B', 4, 0), ('B', 3, -1), ('B', 3, 1), ('A', 4, -1), ('A', 3, 2), ('A', 4, 0), ('B', -3, 2),
    ('B', 2, 2), ('C', -3, 0), ('A', 4, 2), ('A', 4, 1), ('C', -3, 1), ('B', 4, 1), ('B', 4, -1),
    ('C', 2, 0), ('C', 2, 1), ('B', 3, 2), ('C', 3, 0), ('C', 3, 1), ('B', 4, 2), ('C', 4, 0), ('C',
    4, 1))
EXPERT_STEPS = (('own', 0), ('own', 1), ('own', 2), ('near', 0, -1), ('near', 0, 1), ('near', 1, -1), ('near', 1,
    1), ('own', 4), ('near', 2, -1), ('near', 2, 1), ('own', 3), ('far', 0), ('own', 6), ('far', 1),
    ('near', 4, -1), ('near', 4, 1), ('sort', 0), ('own', 5), ('far', 2), ('up', 0, 0), ('near', 3,
    1), ('up', 0, 1), ('near', 3, -1), ('down', 0, 0), ('near', 6, 1), ('down', 0, 1), ('near', 6,
    -1), ('own', 7), ('near', 5, 1), ('far', 4), ('far', 3), ('near', 5, -1), ('rfar', 0), ('near', 7,
    1), ('far', 6), ('sort', 1), ('up', 1, 0), ('near', 7, -1), ('far', 5), ('up', 1, 1), ('down', 1,
    0), ('rnear', 0, 0), ('rnear', 0, 1), ('down', 1, 1), ('sort', 2), ('far', 7), ('up', 2, 0),
    ('up', 2, 1), ('down', 2, 0), ('down', 2, 1), ('rfar', 1), ('sort', 3), ('up', 3, 0), ('back', 0),
    ('up', 3, 1), ('down', 3, 0), ('rfar', 2), ('down', 3, 1), ('rnear', 1, 0), ('rnear', 1, 1),
    ('rfar', 3), ('rnear', 2, 0), ('rnear', 2, 1), ('back', 1), ('rnear', 3, 0), ('rnear', 3, 1),
    ('back', 2), ('back', 3))


def rms_scale(values, norm_gain):
    return (
        values * lax.rsqrt(jnp.mean(values * values, axis=-1, keepdims=True) + NORM_EPS) * norm_gain
    )


EXPERTS, CAP = 32, 4
BACK = (0, 1, -1, 2, -2, 3, -3, 4)


def turn_tables():
    freq_count = HEAD_WIDTH // 4
    frequency = np.power(ROPE_BASE, -np.arange(freq_count) / freq_count).astype(np.float32)
    place = np.arange(N_SP * SEQ // GRID_W, dtype=np.float32)
    angles = np.tile(place[:, None] * frequency, (1, 4)).astype(np.float64)
    sign = np.where((np.arange(HEAD_WIDTH) // freq_count) % 2 == 0, -1.0, 1.0)
    return jnp.asarray(np.stack([np.cos(angles), np.sin(angles) * sign]).astype(np.float32))


def turned(values, gain, cos, sin):
    normed = rms_scale(values, gain)
    lane = lax.broadcasted_iota(jnp.int32, normed.shape, 1)
    partner = jnp.where(
        lane % 64 < 32, pltpu.roll(normed, 96, 1), pltpu.roll(normed, 32, 1)
    )
    return (normed * cos + partner * sin).astype(jnp.bfloat16)


def iota(shape, dim):
    return lax.broadcasted_iota(jnp.int32, shape, dim)


def layer_kernel(
    q_hbm, k_hbm, v_hbm, qg_hbm, kg_hbm, table_hbm, w_hbm, x_hbm, fg_hbm, routing_hbm, scores_hbm,
    gate_hbm, up_hbm, down_hbm,
    out_ref,
    q_ref, k_ref, qg_ref, kg_ref, table_ref, x_ref, fg_ref, routing_ref, scores_ref,
    wg, wu, wd,
    kv, qs, m_ref, l_ref, acc, wfull, att, att_in,
    slots, rows_in, xr, hidden, parts, parts_in, near_out, far_in, near_in, back, returned, middle_ref,
    send_sem, recv_a, recv_b, recv_w, recv_att, load_sem,
    recv_x, recv_part, recv_far, recv_near, recv_back,
):
    sp = lax.axis_index("sp")
    tp = lax.axis_index("tp")
    z, x = sp // NX, sp % NX
    y, c = tp // 2, tp % 2

    def sp_of(dz, dx):
        return ((z - dz + 2 * NZ) % NZ) * NX + (x - dx + 2 * NX) % NX

    def tp_of(dy, other=False):
        return ((y + dy + NY) % NY) * 2 + ((1 - c) if other else c)

    loads = {}
    for n, (name, src, dst) in enumerate((
        ("k", k_hbm, k_ref), ("v", v_hbm, kv.at[sp, :, pl.ds(128, 128)]), ("kg", kg_hbm, kg_ref),
        ("table", table_hbm, table_ref), ("q", q_hbm, q_ref), ("qg", qg_hbm, qg_ref),
        ("w", w_hbm, wfull.at[tp]), ("x", x_hbm, x_ref), ("fg", fg_hbm, fg_ref),
        ("routing", routing_hbm, routing_ref), ("scores", scores_hbm, scores_ref),
        ("gate", gate_hbm.at[0], wg), ("up", up_hbm.at[0], wu), ("down", down_hbm.at[0], wd),
    )):
        loads[name] = pltpu.make_async_copy(src, dst, load_sem.at[n])
        loads[name].start()

    barrier = pltpu.get_barrier_semaphore()

    def greet(i, carry):
        pl.semaphore_signal(barrier, inc=1, device_id=((sp + i) % N_SP, tp), device_id_type=MESH)
        return carry

    lax.fori_loop(1, N_SP, greet, 0)

    def greet_tp(i, carry):
        pl.semaphore_signal(barrier, inc=1, device_id=(sp, (tp + i) % N_TP), device_id_type=MESH)
        return carry

    lax.fori_loop(1, N_TP, greet_tp, 0)

    for name in ("k", "v", "kg", "table"):
        loads[name].wait()

    def table(which):
        lane = iota((GRID_W, 128), 1)
        cols = table_ref[which, 0:GRID_W, :]
        return jnp.concatenate(
            [
                jnp.where(lane < 64, table_ref[which, pl.ds(sp * (SEQ // GRID_W) + i, 1), :], cols)
                for i in range(SEQ // GRID_W)
            ],
            axis=0,
        )

    cos, sin = table(0), table(1)
    kv[sp, :, 0:128] = turned(k_ref[...].astype(jnp.float32), kg_ref[...], cos, sin)
    loads["q"].wait()
    loads["qg"].wait()
    for h in range(2):
        qs[h] = turned(
            q_ref[:, h * 128 : (h + 1) * 128].astype(jnp.float32), qg_ref[...], cos, sin
        )
    m_ref[...] = jnp.full(m_ref.shape, NEG_LARGE, jnp.float32)
    l_ref[...] = jnp.zeros(l_ref.shape, jnp.float32)
    acc[...] = jnp.zeros(acc.shape, jnp.float32)
    pl.semaphore_wait(barrier, N_SP + N_TP - 2)

    sent = []

    def send(src, dst, recv, dev):
        copy = pltpu.make_async_remote_copy(
            src_ref=src, dst_ref=dst, send_sem=send_sem.at[len(sent)], recv_sem=recv,
            device_id=dev, device_id_type=MESH,
        )
        copy.start()
        sent.append(copy)

    def arrived(ref, recv):
        pltpu.make_async_remote_copy(
            src_ref=ref, dst_ref=ref, send_sem=send_sem.at[0], recv_sem=recv,
            device_id=(sp, tp_of(0, True)), device_id_type=MESH,
        ).wait_recv()

    def piece(half, owner):
        if half == "A":
            return kv.at[owner, pl.ds(0, ROWS_A)], recv_a.at[owner]
        return kv.at[owner, pl.ds(ROWS_A, SEQ - ROWS_A)], recv_b.at[owner]

    def pass_on(half, dz, dx, link):
        ref, recv = piece(half, sp_of(dz, dx))
        dev = {
            "z+": (sp_of(-1, 0), tp), "z-": (sp_of(1, 0), tp),
            "x+": (sp_of(0, -1), tp), "x-": (sp_of(0, 1), tp), "x2": (sp_of(0, 2), tp),
        }[link]
        send(ref, ref, recv, dev)

    def next_links(half, dz, dx):
        if half == "A":
            if dz == 0:
                return ["z+", "z-"]
            if dz in (1, 2) or (dz == 3 and dx in (0, 1)):
                return ["z+"]
            if dz in (-1, -2) or (dz == -3 and dx in (-1, 2)):
                return ["z-"]
            return []
        if dx == 0:
            along = ["z+"] if dz in (1, 2, 3) else ["z-"] if dz in (-1, -2) else []
            return along + ["x+", "x-"]
        if dx == 1 and dz % 2 == 0:
            return ["x+"]
        if dx == -1 and dz % 2 == 1:
            return ["x-"]
        return []

    def w_half(owner, half):
        return wfull.at[owner, pl.ds(half * 128, 128)], recv_w.at[owner, half]

    for half, dz, dx, link in (
        ("B", 0, 0, "z+"), ("B", 0, 0, "z-"), ("A", 0, 0, "x+"), ("A", 0, 0, "x-"),
        ("A", 0, 0, "x2"), ("B", 0, 0, "x+"), ("B", 0, 0, "x-"), ("A", 0, 0, "z+"),
        ("A", 0, 0, "z-"),
    ):
        pass_on(half, dz, dx, link)
    for half, dev in ((0, tp_of(1)), (1, tp_of(-1)), (1, tp_of(1)), (0, tp_of(-1))):
        dst, recv = w_half(tp, half)
        send(w_hbm.at[pl.ds(half * 128, 128)], dst, recv, (sp, dev))
    for half in (0, 1):
        dst, recv = w_half(tp, half)
        send(w_hbm.at[pl.ds(half * 128, 128)], dst, recv, (sp, tp_of(0, True)))

    def w_event(dy, half, links):
        ref, recv = w_half(tp_of(dy), half)
        arrived(ref, recv)
        for link in links:
            dev = tp_of(0, True) if link == 0 else tp_of(link)
            send(ref, ref, recv, (sp, dev))

    scale2 = HEAD_WIDTH ** (-0.5) * LOG2E

    def attend(group, i):
        block = kv[pl.ds(group * NX + 2 * i, 2)].reshape(2 * SEQ, 256)
        keys, values = block[:, 0:128], block[:, 128:256]
        for h in range(2):
            s = lax.dot_general(
                qs[h], keys, (((1,), (1,)), ((), ())), preferred_element_type=jnp.float32
            )
            m_old = m_ref[h]
            m_new = jnp.maximum(m_old, jnp.max(s, axis=1, keepdims=True))
            alpha = jnp.exp2((m_old - m_new) * scale2)
            m_all = jnp.concatenate([m_new * scale2] * 4, axis=1)
            p = jnp.exp2(s * scale2 - m_all)
            l_ref[h] = l_ref[h] * alpha + (
                (p[:, 0:128] + p[:, 128:256]) + (p[:, 256:384] + p[:, 384:512])
            )
            acc[h] = acc[h] * alpha + jnp.dot(
                p.astype(jnp.bfloat16), values, preferred_element_type=jnp.float32
            )
            m_ref[h] = m_new

    w_plan = {30: ((-1, 0, (1, 0)), (1, 1, (-1, 0))), 70: ((-1, 1, (0,)), (1, 0, (0,)))}
    for count, (half, dz, dx) in enumerate(ATTENTION_STEPS):
        if half == "C":
            attend((z - dz + NZ) % NZ, dx)
        else:
            ref, recv = piece(half, sp_of(dz, dx))
            arrived(ref, recv)
            for link in next_links(half, dz, dx):
                pass_on(half, dz, dx, link)
        for dy, w_part, links in w_plan.get(count, ()):
            w_event(dy, w_part, links)

    for h in range(2):
        total = jnp.sum(l_ref[h], axis=1, keepdims=True)
        att[:, h * 128 : (h + 1) * 128] = (acc[h] / total).astype(jnp.bfloat16)

    att_in[tp] = att[pl.ds(tp * 32, 32), :]
    for dy, other in ((0, True), (1, False), (1, True), (3, False), (3, True), (2, False), (2, True)):
        to = tp_of(dy, other)
        send(att.at[pl.ds(to * 32, 32)], att_in.at[tp], recv_att.at[tp], (sp, to))

    for name in ("routing", "scores"):
        loads[name].wait()
    expert_no = iota((EXPERTS, 32), 0)
    first = (routing_ref[0:1, :] == expert_no).astype(jnp.float32)
    second = (routing_ref[1:2, :] == expert_no).astype(jnp.float32)
    top = jnp.maximum(scores_ref[0:1, :], scores_ref[1:2, :])
    e0, e1 = jnp.exp(scores_ref[0:1, :] - top), jnp.exp(scores_ref[1:2, :] - top)
    gates = first * (e0 / (e0 + e1)) + second * (e1 / (e0 + e1))
    named = first + second
    before = (iota((32, 32), 0) < iota((32, 32), 1)).astype(jnp.bfloat16)
    rank = jnp.dot(named.astype(jnp.bfloat16), before, preferred_element_type=jnp.float32)
    slot = jnp.where(named > 0.5, rank, -1.0).astype(jnp.bfloat16)
    again = (iota((32, 128), 1) % 32 == iota((32, 128), 0)).astype(jnp.bfloat16)
    slot4 = jnp.dot(slot, again, preferred_element_type=jnp.float32).astype(jnp.bfloat16)
    gates4 = jnp.dot(
        gates, again.astype(jnp.float32), preferred_element_type=jnp.float32,
        precision=lax.Precision.HIGHEST,
    )
    spread = (iota((512, EXPERTS), 0) // 16 == iota((512, EXPERTS), 1)).astype(jnp.bfloat16)
    slot_rows = jnp.dot(spread, slot4, preferred_element_type=jnp.float32)
    row = iota((512, 128), 0)
    held = (slot_rows == (row % 4).astype(jnp.float32)) & (
        (row // 4) % 4 == iota((512, 128), 1) // 32
    )
    pick = held.astype(jnp.bfloat16)
    merge_rows = jnp.where(
        held,
        jnp.dot(
            spread.astype(jnp.float32), gates4, preferred_element_type=jnp.float32,
            precision=lax.Precision.HIGHEST,
        ),
        0.0,
    )
    merge = merge_rows.T

    for name in ("w", "x", "fg"):
        loads[name].wait()
    w_event(2, 0, (0,))
    w_event(2, 1, (0,))
    total = jnp.zeros((32, 2048), jnp.float32)
    order = [(0, False), (1, False), (3, False), (2, False), (0, True), (1, True), (3, True), (2, True)]
    for dy, other in order:
        owner = tp_of(dy, other)
        if (dy, other) != (0, False):
            arrived(att_in.at[owner], recv_att.at[owner])
        if other:
            for half in (0, 1):
                ref, recv = w_half(owner, half)
                arrived(ref, recv)
        part = jnp.dot(att_in[owner], wfull[owner], preferred_element_type=jnp.float32)
        total = total + part.astype(jnp.bfloat16).astype(jnp.float32)
    middle = x_ref[...].astype(jnp.float32) + total.astype(jnp.bfloat16).astype(jnp.float32)
    middle_ref[...] = middle
    normed = rms_scale(middle, fg_ref[...]).astype(jnp.bfloat16)

    stacked = jnp.concatenate([normed[:, 512 * j : 512 * (j + 1)] for j in range(4)], axis=0)
    slots[...] = (
        jnp.dot(pick, stacked, preferred_element_type=jnp.float32)
        .astype(jnp.bfloat16)
        .reshape(EXPERTS, 16, 512)
    )
    rows_in[tp, 0, x] = slots[sp]
    for g, dz in enumerate(BACK):
        for dx in (0, 1, -1, 2):
            if (dz, dx) != (0, 0):
                to = sp_of(-dz, -dx)
                send(slots.at[to], rows_in.at[tp, g, x], recv_x.at[tp, g], (to, tp))

    out_no, in_no = iota((128, 128), 0), iota((128, 128), 1)
    sort = (
        in_no == (out_no % 32 // 4) * 16 + (out_no // 32) * 4 + out_no % 4
    ).astype(jnp.bfloat16)
    out_no, in_no = in_no, out_no
    unsort = (
        in_no == (out_no % 32 // 4) * 16 + (out_no // 32) * 4 + out_no % 4
    ).astype(jnp.bfloat16)

    def group_of(owner, g):
        return rows_in.at[owner, g], recv_x.at[owner, g]

    def spread_rows(owner, g, links):
        ref, recv = group_of(owner, g)
        for link in links:
            dev = tp_of(0, True) if link == 0 else tp_of(link)
            send(ref, ref, recv, (sp, dev))

    def own(g):
        ref, recv = group_of(tp, g)
        arrived(rows_in.at[tp, g, pl.ds(0, 3)] if g == 0 else ref, recv)
        spread_rows(tp, g, (1, -1, 0))

    def near(g, dy):
        owner = tp_of(dy)
        arrived(*group_of(owner, g))
        spread_rows(owner, g, ((-dy, 0) if (g % 2 == 0) == (dy == -1) else (0,)))

    def far(g):
        owner = tp_of(2)
        arrived(*group_of(owner, g))
        spread_rows(owner, g, (0,))

    def sort_rows(o):
        for g in (2 * o, 2 * o + 1):
            for dy in (0, -1, 1, 2):
                arrived(*group_of(tp_of(dy, True), g))

        def sorted_rows(t, carry):
            block = rows_in[t, pl.ds(2 * o, 2)].reshape(128, 512)
            out = jnp.dot(sort, block, preferred_element_type=jnp.float32).astype(jnp.bfloat16)
            at = pl.ds(pl.multiple_of(t * 32, 32), 32)
            for j in range(4):
                xr[at, 512 * j : 512 * (j + 1)] = out[32 * j : 32 * (j + 1)]
            return carry

        lax.fori_loop(0, N_TP, sorted_rows, 0)

    def up(o, n):
        if (o, n) == (0, 0):
            for name in ("gate", "up", "down"):
                loads[name].wait()
        cols = slice(256 * n, 256 * (n + 1))
        gate_part = jnp.dot(xr[...], wg[:, cols], preferred_element_type=jnp.float32)
        up_part = jnp.dot(xr[...], wu[:, cols], preferred_element_type=jnp.float32)
        hidden[:, cols] = (gate_part / (1.0 + jnp.exp(-gate_part)) * up_part).astype(jnp.bfloat16)

    def down(o, n):
        for j in (2 * n, 2 * n + 1):
            cols = slice(512 * j, 512 * (j + 1))
            part = jnp.dot(hidden[...], wd[:, cols], preferred_element_type=jnp.float32)
            parts[o, :, :, cols] = part.astype(jnp.bfloat16).reshape(N_TP, 32, 512)
        if (o, n) not in last_down:
            return
        for dy in (2, 1, -1, 0):
            home = (y + dy + NY) % NY
            send(
                parts.at[o, tp_of(dy, True)], parts_in.at[o, home], recv_part.at[o, home],
                (sp, tp_of(0, True)),
            )

    from_partner = set()

    def chip_sum(o, dy):
        home = (y + dy + NY) % NY
        if (o, dy) not in from_partner:
            arrived(parts_in.at[o, home], recv_part.at[o, home])
            from_partner.add((o, dy))
        return parts[o, tp_of(dy)].astype(jnp.float32) + parts_in[o, home].astype(jnp.float32)

    def reduce_far(o):
        near_out[o, 0] = chip_sum(o, 2).astype(jnp.bfloat16)
        send(near_out.at[o, 0, pl.ds(0, 16)], far_in.at[o, 0], recv_far.at[o, 0], (sp, tp_of(1)))
        send(near_out.at[o, 0, pl.ds(16, 16)], far_in.at[o, 1], recv_far.at[o, 1], (sp, tp_of(-1)))

    def reduce_near(o, n):
        dy = (1, -1)[n]
        mine = chip_sum(o, dy)
        arrived(far_in.at[o, n], recv_far.at[o, n])
        at = slice(16 * n, 16 * n + 16)
        rest = slice(16 - 16 * n, 32 - 16 * n)
        near_out[o, 1 + n, at, :] = (mine[at] + far_in[o, n].astype(jnp.float32)).astype(
            jnp.bfloat16
        )
        near_out[o, 1 + n, rest, :] = mine[rest].astype(jnp.bfloat16)
        send(near_out.at[o, 1 + n], near_in.at[o, n], recv_near.at[o, n], (sp, tp_of(dy)))

    def give_back(o):
        whole = chip_sum(o, 0)
        for n in (0, 1):
            arrived(near_in.at[o, n], recv_near.at[o, n])
            whole = whole + near_in[o, n].astype(jnp.float32)
        result = whole.astype(jnp.bfloat16)
        stack = jnp.concatenate([result[:, 512 * j : 512 * (j + 1)] for j in range(4)], axis=0)
        back[o] = (
            jnp.dot(unsort, stack, preferred_element_type=jnp.float32)
            .astype(jnp.bfloat16)
            .reshape(8, 16, 512)
        )
        if o == 0:
            returned[sp] = back[0, x]
        for n in (0, 1):
            dz = BACK[2 * o + n]
            for dx in (0, 1, -1, 2):
                if (dz, dx) != (0, 0):
                    to = sp_of(dz, dx)
                    send(back.at[o, 4 * n + to % NX], returned.at[sp], recv_back, (to, tp))

    last_down = {}
    for kind, o, *n in EXPERT_STEPS:
        if kind == "down":
            last_down[o] = n[0]
    last_down = set(last_down.items())
    steps = dict(
        own=own, near=near, far=far, sort=sort_rows, up=up, down=down, rfar=reduce_far,
        rnear=reduce_near, back=give_back,
    )
    for kind, *args in EXPERT_STEPS:
        steps[kind](*args)

    arrived(returned.at[pl.ds(0, N_SP - 1)], recv_back)
    results = returned[...].reshape(512, 512)
    routed = jnp.dot(
        merge, results.astype(jnp.float32), preferred_element_type=jnp.float32,
        precision=lax.Precision.HIGHEST,
    )
    for j in range(4):
        cols = slice(512 * j, 512 * (j + 1))
        out_ref[:, cols] = (middle_ref[:, cols] + routed[32 * j : 32 * (j + 1)]).astype(jnp.bfloat16)
    for copy in sent:
        copy.wait_send()


def local(
    x_resid,
    query_proj,
    projected_key_heads,
    projected_value_heads,
    query_gain,
    key_norm_gain,
    out_weight,
    ffn_gain,
    routing,
    route_scores,
    expert_gate,
    expert_up,
    expert_down,
):
    hbm = pl.BlockSpec(memory_space=pltpu.HBM)
    bf16, f32 = jnp.bfloat16, jnp.float32
    dma = pltpu.SemaphoreType.DMA
    return pl.pallas_call(
        layer_kernel,
        out_shape=jax.ShapeDtypeStruct((32, 2048), bf16),
        in_specs=[hbm] * 14,
        out_specs=pl.BlockSpec(memory_space=pltpu.VMEM),
        scratch_shapes=[
            pltpu.VMEM((SEQ, 256), bf16),
            pltpu.VMEM((SEQ, 128), bf16),
            pltpu.VMEM((1, 128), f32),
            pltpu.VMEM((1, 128), f32),
            pltpu.VMEM((2, 128, 128), f32),
            pltpu.VMEM((32, 2048), bf16),
            pltpu.VMEM((1, 2048), f32),
            pltpu.VMEM((2, 32), jnp.int32),
            pltpu.VMEM((2, 32), f32),
            pltpu.VMEM((2048, 512), bf16),
            pltpu.VMEM((2048, 512), bf16),
            pltpu.VMEM((512, 2048), bf16),
            pltpu.VMEM((N_SP, SEQ, 256), bf16),
            pltpu.VMEM((2, SEQ, 128), bf16),
            pltpu.VMEM((2, SEQ, 128), f32),
            pltpu.VMEM((2, SEQ, 128), f32),
            pltpu.VMEM((2, SEQ, 128), f32),
            pltpu.VMEM((N_TP, 256, 2048), bf16),
            pltpu.VMEM((SEQ, 256), bf16),
            pltpu.VMEM((N_TP, 32, 256), bf16),
            pltpu.VMEM((EXPERTS, 16, 512), bf16),
            pltpu.VMEM((N_TP, 8, NX, 16, 512), bf16),
            pltpu.VMEM((256, 2048), bf16),
            pltpu.VMEM((256, 512), bf16),
            pltpu.VMEM((4, N_TP, 32, 2048), bf16),
            pltpu.VMEM((4, NY, 32, 2048), bf16),
            pltpu.VMEM((4, 3, 32, 2048), bf16),
            pltpu.VMEM((4, 2, 16, 2048), bf16),
            pltpu.VMEM((4, 2, 32, 2048), bf16),
            pltpu.VMEM((4, 8, 16, 512), bf16),
            pltpu.VMEM((EXPERTS, 16, 512), bf16),
            pltpu.VMEM((32, 2048), f32),
            dma((256,)),
            dma((N_SP,)),
            dma((N_SP,)),
            dma((N_TP, 2)),
            dma((N_TP,)),
            dma((14,)),
            dma((N_TP, 8)),
            dma((4, NY)),
            dma((4, 2)),
            dma((4, 2)),
            dma,
        ],
        compiler_params=pltpu.CompilerParams(
            collective_id=0, has_side_effects=True, vmem_limit_bytes=60 * 1024 * 1024
        ),
        name="layer",
    )(
        query_proj, projected_key_heads, projected_value_heads,
        query_gain.reshape(1, -1), key_norm_gain.reshape(1, -1), turn_tables(), out_weight, x_resid,
        ffn_gain.reshape(1, -1), routing.T, route_scores.T, expert_gate, expert_up, expert_down,
    )


def solution(mesh):
    in_specs = (
        P(("sp", "tp"), None),
        P("sp", "tp"),
        P("sp", "tp"),
        P("sp", "tp"),
        P(),
        P(),
        P("tp", None),
        P(),
        P(("sp", "tp"), None),
        P(("sp", "tp"), None),
        P("sp", None, "tp"),
        P("sp", None, "tp"),
        P("sp", "tp", None),
    )
    out_specs = P(("sp", "tp"), None)
    return jax.shard_map(local, mesh=mesh, in_specs=in_specs, out_specs=out_specs, check_vma=False)
```

```python
import functools
import jax
import jax.numpy as jnp
import numpy as np
from jax import lax
from jax.experimental import pallas as pl
from jax.experimental.pallas import tpu as pltpu
from jax.sharding import PartitionSpec as P

HEAD_WIDTH = 128
TOP = 2
GRID_W = 64
NORM_EPS = 1e-06
ROPE_BASE = 10000.0
NEG_LARGE = -1e30
LOG2E = 1.4426950408889634
MESH = pl.DeviceIdType.MESH

NZ, NX, NY = 8, 4, 4
N_SP = NZ * NX
N_TP = NY * 2
SEQ = 256
ROWS_A = 96
ATTENTION_STEPS = (('A', 0, -1), ('A', 0, 1), ('B', -1, 0), ('B', 1, 0), ('A', 0, 2), ('A', -1, 0), ('A', 1, 0),
    ('B', 0, -1), ('A', -1, -1), ('A', 1, -1), ('B', 0, 1), ('A', -1, 1), ('A', 1, 1), ('B', -1, -1),
    ('B', -1, 1), ('B', -2, 0), ('B', 2, 0), ('B', 1, -1), ('A', -1, 2), ('A', 1, 2), ('B', 1, 1),
    ('A', -2, 0), ('A', 2, 0), ('B', -1, 2), ('C', -1, 0), ('A', -2, -1), ('A', 2, -1), ('B', 0, 2),
    ('C', -1, 1), ('A', -2, 1), ('A', 2, 1), ('B', -2, -1), ('C', 0, 0), ('B', -2, 1), ('C', 0, 1),
    ('B', -3, 0), ('B', 3, 0), ('B', 2, -1), ('B', 2, 1), ('A', -2, 2), ('A', 2, 2), ('B', 1, 2),
    ('C', 1, 0), ('A', 3, 0), ('A', -3, 0), ('C', 1, 1), ('A', -3, -1), ('A', 3, -1), ('B', -2, 2),
    ('C', -2, 0), ('A', 3, 1), ('B', -3, -1), ('A', -3, 1), ('C', -2, 1), ('A', -3, 2), ('B', -3, 1),
    ('B', 4, 0), ('B', 3, -1), ('B', 3, 1), ('A', 4, -1), ('A', 3, 2), ('A', 4, 0), ('B', -3, 2),
    ('B', 2, 2), ('C', -3, 0), ('A', 4, 2), ('A', 4, 1), ('C', -3, 1), ('B', 4, 1), ('B', 4, -1),
    ('C', 2, 0), ('C', 2, 1), ('B', 3, 2), ('C', 3, 0), ('C', 3, 1), ('B', 4, 2), ('C', 4, 0), ('C',
    4, 1))
EXPERT_STEPS = (('own', 0), ('own', 1), ('own', 3), ('near', 0, -1), ('near', 0, 1), ('near', 1, -1), ('near', 1,
    1), ('own', 4), ('near', 3, -1), ('near', 3, 1), ('own', 2), ('far', 0), ('own', 5), ('far', 1),
    ('near', 4, -1), ('near', 4, 1), ('near', 2, -1), ('own', 6), ('far', 3), ('near', 5, -1),
    ('sort', 0), ('near', 2, 1), ('up', 0, 0), ('own', 7), ('far', 4), ('up', 0, 1), ('near', 5, 1),
    ('down', 0, 0), ('far', 2), ('down', 0, 1), ('near', 6, 1), ('near', 6, -1), ('near', 7, 1),
    ('near', 7, -1), ('far', 5), ('sort', 1), ('rfar', 0), ('up', 1, 0), ('far', 6), ('up', 1, 1),
    ('far', 7), ('down', 1, 0), ('down', 1, 1), ('sort', 2), ('rnear', 0, 0), ('rnear', 0, 1), ('up',
    2, 0), ('up', 2, 1), ('down', 2, 0), ('down', 2, 1), ('rfar', 1), ('sort', 3), ('up', 3, 0),
    ('up', 3, 1), ('down', 3, 0), ('down', 3, 1), ('back', 0), ('rfar', 2), ('rnear', 1, 0), ('rnear',
    1, 1), ('rfar', 3), ('rnear', 2, 0), ('rnear', 2, 1), ('back', 1), ('rnear', 3, 0), ('rnear', 3,
    1), ('back', 2), ('back', 3))


def rms_scale(values, norm_gain):
    return (
        values * lax.rsqrt(jnp.mean(values * values, axis=-1, keepdims=True) + NORM_EPS) * norm_gain
    )


EXPERTS, CAP = 32, 4
BACK = (0, 1, 2, -1, -2, -3, 3, 4)
AHEAD = (0, 1, -1, 2, -2, 3, -3, 4)
KINDS = ("A", "B", "w", "att", "slots", "rows", "parts", "far", "near", "back")


def turn_tables():
    freq_count = HEAD_WIDTH // 4
    frequency = np.power(ROPE_BASE, -np.arange(freq_count) / freq_count).astype(np.float32)
    place = np.arange(N_SP * SEQ // GRID_W, dtype=np.float32)
    angles = np.tile(place[:, None] * frequency, (1, 4)).astype(np.float64)
    sign = np.where((np.arange(HEAD_WIDTH) // freq_count) % 2 == 0, -1.0, 1.0)
    return jnp.asarray(np.stack([np.cos(angles), np.sin(angles) * sign]).astype(np.float32))


def turned(values, gain, cos, sin):
    normed = rms_scale(values, gain)
    lane = lax.broadcasted_iota(jnp.int32, normed.shape, 1)
    partner = jnp.where(
        lane % 64 < 32, pltpu.roll(normed, 96, 1), pltpu.roll(normed, 32, 1)
    )
    return (normed * cos + partner * sin).astype(jnp.bfloat16)


def iota(shape, dim):
    return lax.broadcasted_iota(jnp.int32, shape, dim)


def layer_kernel(
    q_hbm, k_hbm, v_hbm, qg_hbm, kg_hbm, table_hbm, w_hbm, x_hbm, fg_hbm, routing_hbm, scores_hbm,
    gate_hbm, up_hbm, down_hbm,
    out_ref,
    q_ref, k_ref, qg_ref, kg_ref, table_ref, x_ref, fg_ref, routing_ref, scores_ref,
    wg, wu, wd,
    kv, qs, m_ref, l_ref, acc, wfull, att, att_in,
    slots, rows_in, xr, hidden, parts, parts_in, near_out, far_in, near_in, back, returned, middle_ref,
    send_sem, recv_a, recv_b, recv_w, recv_att, load_sem,
    recv_own, recv_y, recv_other, recv_part, recv_far, recv_near, recv_back,
):
    sp = lax.axis_index("sp")
    tp = lax.axis_index("tp")
    z, x = sp // NX, sp % NX
    y, c = tp // 2, tp % 2

    def sp_of(dz, dx):
        return ((z - dz + 2 * NZ) % NZ) * NX + (x - dx + 2 * NX) % NX

    def tp_of(dy, other=False):
        return ((y + dy + NY) % NY) * 2 + ((1 - c) if other else c)

    loads = {}
    for n, (name, src, dst) in enumerate((
        ("k", k_hbm, k_ref), ("v", v_hbm, kv.at[sp, :, pl.ds(128, 128)]), ("kg", kg_hbm, kg_ref),
        ("table", table_hbm, table_ref), ("q", q_hbm, q_ref), ("qg", qg_hbm, qg_ref),
        ("w", w_hbm, wfull.at[tp]), ("x", x_hbm, x_ref), ("fg", fg_hbm, fg_ref),
        ("routing", routing_hbm, routing_ref), ("scores", scores_hbm, scores_ref),
        ("gate", gate_hbm.at[0], wg), ("up", up_hbm.at[0], wu), ("down", down_hbm.at[0], wd),
    )):
        loads[name] = pltpu.make_async_copy(src, dst, load_sem.at[n])
        loads[name].start()

    barrier = pltpu.get_barrier_semaphore()

    friends = [(sp_of(dz, dx), tp) for dz, dx in ((1, 0), (-1, 0), (0, 1), (0, -1), (0, 2))]
    for dev in friends:
        pl.semaphore_signal(barrier, inc=1, device_id=dev, device_id_type=MESH)

    def greet_tp(i, carry):
        pl.semaphore_signal(barrier, inc=1, device_id=(sp, (tp + i) % N_TP), device_id_type=MESH)
        return carry

    lax.fori_loop(1, N_TP, greet_tp, 0)

    for name in ("k", "v", "kg", "table"):
        loads[name].wait()

    def table(which):
        lane = iota((GRID_W, 128), 1)
        cols = table_ref[which, 0:GRID_W, :]
        return jnp.concatenate(
            [
                jnp.where(lane < 64, table_ref[which, pl.ds(sp * (SEQ // GRID_W) + i, 1), :], cols)
                for i in range(SEQ // GRID_W)
            ],
            axis=0,
        )

    cos, sin = table(0), table(1)
    kv[sp, :, 0:128] = turned(k_ref[...].astype(jnp.float32), kg_ref[...], cos, sin)
    loads["q"].wait()
    loads["qg"].wait()
    for h in range(2):
        qs[h] = turned(
            q_ref[:, h * 128 : (h + 1) * 128].astype(jnp.float32), qg_ref[...], cos, sin
        )
    m_ref[...] = jnp.full(m_ref.shape, NEG_LARGE, jnp.float32)
    l_ref[...] = jnp.zeros(l_ref.shape, jnp.float32)
    acc[...] = jnp.zeros(acc.shape, jnp.float32)
    pl.semaphore_wait(barrier, len(friends) + N_TP - 1)

    def send(kind, src, dst, recv, dev):
        pltpu.make_async_remote_copy(
            src_ref=src, dst_ref=dst, send_sem=send_sem.at[KINDS.index(kind)], recv_sem=recv,
            device_id=dev, device_id_type=MESH,
        ).start()

    def arrived(ref, recv):
        pltpu.make_async_remote_copy(
            src_ref=ref, dst_ref=ref, send_sem=send_sem.at[0], recv_sem=recv,
            device_id=(sp, tp_of(0, True)), device_id_type=MESH,
        ).wait_recv()

    def all_sent(kind, ref):
        pltpu.make_async_remote_copy(
            src_ref=ref, dst_ref=ref, send_sem=send_sem.at[KINDS.index(kind)],
            recv_sem=recv_back, device_id=(sp, tp_of(0, True)), device_id_type=MESH,
        ).wait_send()

    def piece(half, owner):
        if half == "A":
            return kv.at[owner, pl.ds(0, ROWS_A)], recv_a.at[owner]
        return kv.at[owner, pl.ds(ROWS_A, SEQ - ROWS_A)], recv_b.at[owner]

    def pass_on(half, dz, dx, link):
        ref, recv = piece(half, sp_of(dz, dx))
        dev = {
            "z+": (sp_of(-1, 0), tp), "z-": (sp_of(1, 0), tp),
            "x+": (sp_of(0, -1), tp), "x-": (sp_of(0, 1), tp), "x2": (sp_of(0, 2), tp),
        }[link]
        send(half, ref, ref, recv, dev)

    def next_links(half, dz, dx):
        if half == "A":
            if dz == 0:
                return ["z+", "z-"]
            if dz in (1, 2) or (dz == 3 and dx in (0, 1)):
                return ["z+"]
            if dz in (-1, -2) or (dz == -3 and dx in (-1, 2)):
                return ["z-"]
            return []
        if dx == 0:
            along = ["z+"] if dz in (1, 2, 3) else ["z-"] if dz in (-1, -2) else []
            return along + ["x+", "x-"]
        if dx == 1 and dz % 2 == 0:
            return ["x+"]
        if dx == -1 and dz % 2 == 1:
            return ["x-"]
        return []

    def w_half(owner, half):
        return wfull.at[owner, pl.ds(half * 128, 128)], recv_w.at[owner, half]

    for half, dz, dx, link in (
        ("B", 0, 0, "z+"), ("B", 0, 0, "z-"), ("A", 0, 0, "x+"), ("A", 0, 0, "x-"),
        ("A", 0, 0, "x2"), ("B", 0, 0, "x+"), ("B", 0, 0, "x-"), ("A", 0, 0, "z+"),
        ("A", 0, 0, "z-"),
    ):
        pass_on(half, dz, dx, link)
    for half, dev in ((0, tp_of(1)), (1, tp_of(-1)), (1, tp_of(1)), (0, tp_of(-1))):
        dst, recv = w_half(tp, half)
        send("w", w_hbm.at[pl.ds(half * 128, 128)], dst, recv, (sp, dev))
    for half in (0, 1):
        dst, recv = w_half(tp, half)
        send("w", w_hbm.at[pl.ds(half * 128, 128)], dst, recv, (sp, tp_of(0, True)))

    def w_event(dy, half, links):
        ref, recv = w_half(tp_of(dy), half)
        arrived(ref, recv)
        for link in links:
            dev = tp_of(0, True) if link == 0 else tp_of(link)
            send("w", ref, ref, recv, (sp, dev))

    scale2 = HEAD_WIDTH ** (-0.5) * LOG2E

    def attend(group, i):
        block = kv[pl.ds(group * NX + 2 * i, 2)].reshape(2 * SEQ, 256)
        keys, values = block[:, 0:128], block[:, 128:256]
        for h in range(2):
            s = lax.dot_general(
                qs[h], keys, (((1,), (1,)), ((), ())), preferred_element_type=jnp.float32
            )
            m_old = m_ref[h]
            m_new = jnp.maximum(m_old, jnp.max(s, axis=1, keepdims=True))
            alpha = jnp.exp2((m_old - m_new) * scale2)
            m_all = jnp.concatenate([m_new * scale2] * 4, axis=1)
            p = jnp.exp2(s * scale2 - m_all)
            l_ref[h] = l_ref[h] * alpha + (
                (p[:, 0:128] + p[:, 128:256]) + (p[:, 256:384] + p[:, 384:512])
            )
            acc[h] = acc[h] * alpha + jnp.dot(
                p.astype(jnp.bfloat16), values, preferred_element_type=jnp.float32
            )
            m_ref[h] = m_new

    w_plan = {30: ((-1, 0, (1, 0)), (1, 1, (-1, 0))), 70: ((-1, 1, (0,)), (1, 0, (0,)))}
    for count, (half, dz, dx) in enumerate(ATTENTION_STEPS):
        if half == "C":
            attend((z - dz + NZ) % NZ, dx)
        else:
            ref, recv = piece(half, sp_of(dz, dx))
            arrived(ref, recv)
            for link in next_links(half, dz, dx):
                pass_on(half, dz, dx, link)
        for dy, w_part, links in w_plan.get(count, ()):
            w_event(dy, w_part, links)

    for h in range(2):
        total = jnp.sum(l_ref[h], axis=1, keepdims=True)
        att[:, h * 128 : (h + 1) * 128] = (acc[h] / total).astype(jnp.bfloat16)

    att_in[tp] = att[pl.ds(tp * 32, 32), :]
    for dy, other in ((0, True), (1, False), (1, True), (3, False), (3, True), (2, False), (2, True)):
        to = tp_of(dy, other)
        send("att", att.at[pl.ds(to * 32, 32)], att_in.at[tp], recv_att.at[tp], (sp, to))

    for name in ("routing", "scores"):
        loads[name].wait()
    expert_no = iota((EXPERTS, 32), 0)
    first = (routing_ref[0:1, :] == expert_no).astype(jnp.float32)
    second = (routing_ref[1:2, :] == expert_no).astype(jnp.float32)
    top = jnp.maximum(scores_ref[0:1, :], scores_ref[1:2, :])
    e0, e1 = jnp.exp(scores_ref[0:1, :] - top), jnp.exp(scores_ref[1:2, :] - top)
    gates = first * (e0 / (e0 + e1)) + second * (e1 / (e0 + e1))
    named = first + second
    before = (iota((32, 32), 0) < iota((32, 32), 1)).astype(jnp.bfloat16)
    rank = jnp.dot(named.astype(jnp.bfloat16), before, preferred_element_type=jnp.float32)
    slot = jnp.where(named > 0.5, rank, -1.0).astype(jnp.bfloat16)
    again = (iota((32, 128), 1) % 32 == iota((32, 128), 0)).astype(jnp.bfloat16)
    slot4 = jnp.dot(slot, again, preferred_element_type=jnp.float32).astype(jnp.bfloat16)
    gates4 = jnp.dot(
        gates, again.astype(jnp.float32), preferred_element_type=jnp.float32,
        precision=lax.Precision.HIGHEST,
    )
    spread = (iota((512, EXPERTS), 0) // 16 == iota((512, EXPERTS), 1)).astype(jnp.bfloat16)
    slot_rows = jnp.dot(spread, slot4, preferred_element_type=jnp.float32)
    row = iota((512, 128), 0)
    held = (slot_rows == (row % 4).astype(jnp.float32)) & (
        (row // 4) % 4 == iota((512, 128), 1) // 32
    )
    pick = held.astype(jnp.bfloat16)
    merge_rows = jnp.where(
        held,
        jnp.dot(
            spread.astype(jnp.float32), gates4, preferred_element_type=jnp.float32,
            precision=lax.Precision.HIGHEST,
        ),
        0.0,
    )
    merge = merge_rows.T

    for name in ("w", "x", "fg"):
        loads[name].wait()
    w_event(2, 0, (0,))
    w_event(2, 1, (0,))
    total = jnp.zeros((32, 2048), jnp.float32)
    order = [(0, False), (1, False), (3, False), (2, False), (0, True), (1, True), (3, True), (2, True)]
    for dy, other in order:
        owner = tp_of(dy, other)
        if (dy, other) != (0, False):
            arrived(att_in.at[owner], recv_att.at[owner])
        if other:
            for half in (0, 1):
                ref, recv = w_half(owner, half)
                arrived(ref, recv)
        part = jnp.dot(att_in[owner], wfull[owner], preferred_element_type=jnp.float32)
        total = total + part.astype(jnp.bfloat16).astype(jnp.float32)
    middle = x_ref[...].astype(jnp.float32) + total.astype(jnp.bfloat16).astype(jnp.float32)
    middle_ref[...] = middle
    normed = rms_scale(middle, fg_ref[...]).astype(jnp.bfloat16)

    stacked = jnp.concatenate([normed[:, 512 * j : 512 * (j + 1)] for j in range(4)], axis=0)
    slots[...] = (
        jnp.dot(pick, stacked, preferred_element_type=jnp.float32)
        .astype(jnp.bfloat16)
        .reshape(EXPERTS, 16, 512)
    )
    rows_in[tp, 0, x] = slots[sp]
    for dx in (0, 1, -1, 2):
        to = sp_of(0, -dx)
        for n, dy in ((0, 1), (1, -1)):
            send("rows", slots.at[to], rows_in.at[tp, 0, x], recv_y.at[n, 0], (to, tp_of(dy)))
        if dx != 0:
            send("slots", slots.at[to], rows_in.at[tp, 0, x], recv_own.at[0], (to, tp))
    for dz in AHEAD[1:]:
        for dx in (0, 1, -1, 2):
            to = sp_of(-dz, -dx)
            g = BACK.index(dz)
            send("slots", slots.at[to], rows_in.at[tp, g, x], recv_own.at[g], (to, tp))

    out_no, in_no = iota((128, 128), 0), iota((128, 128), 1)
    sort = (
        in_no == (out_no % 32 // 4) * 16 + (out_no // 32) * 4 + out_no % 4
    ).astype(jnp.bfloat16)
    out_no, in_no = in_no, out_no
    unsort = (
        in_no == (out_no % 32 // 4) * 16 + (out_no // 32) * 4 + out_no % 4
    ).astype(jnp.bfloat16)

    def spread_rows(owner, g, to_far=None):
        ref = rows_in.at[owner, g]
        if to_far is not None:
            send("rows", ref, ref, recv_y.at[2, g], (sp, tp_of(to_far)))
        send("rows", ref, ref, recv_other.at[g // 2], (sp, tp_of(0, True)))

    def own(g):
        ref = rows_in.at[tp, g]
        arrived(rows_in.at[tp, 0, pl.ds(0, 3)] if g == 0 else ref, recv_own.at[g])
        if g != 0:
            for n, dy in ((0, 1), (1, -1)):
                send("rows", ref, ref, recv_y.at[n, g], (sp, tp_of(dy)))
        spread_rows(tp, g)

    def near(g, dy):
        owner = tp_of(dy)
        arrived(rows_in.at[owner, g], recv_y.at[(1 + dy) // 2, g])
        spread_rows(owner, g, -dy if (g % 2 == 0) == (dy == -1) else None)

    def far(g):
        owner = tp_of(2)
        arrived(rows_in.at[owner, g], recv_y.at[2, g])
        spread_rows(owner, g)

    def sort_rows(o):
        arrived(rows_in.at[0], recv_other.at[o])

        for t in range(N_TP):
            block = rows_in[t, 2 * o : 2 * o + 2].reshape(128, 512)
            out = jnp.dot(sort, block, preferred_element_type=jnp.float32).astype(jnp.bfloat16)
            for j in range(4):
                xr[32 * t : 32 * t + 32, 512 * j : 512 * (j + 1)] = out[32 * j : 32 * (j + 1)]

    def up(o, n):
        if (o, n) == (0, 0):
            for name in ("gate", "up", "down"):
                loads[name].wait()
        cols = slice(256 * n, 256 * (n + 1))
        gate_part = jnp.dot(xr[...], wg[:, cols], preferred_element_type=jnp.float32)
        up_part = jnp.dot(xr[...], wu[:, cols], preferred_element_type=jnp.float32)
        hidden[:, cols] = (gate_part / (1.0 + jnp.exp(-gate_part)) * up_part).astype(jnp.bfloat16)

    def down(o, n):
        for j in (2 * n, 2 * n + 1):
            cols = slice(512 * j, 512 * (j + 1))
            part = jnp.dot(hidden[...], wd[:, cols], preferred_element_type=jnp.float32)
            parts[o, :, :, cols] = part.astype(jnp.bfloat16).reshape(N_TP, 32, 512)
        if (o, n) not in last_down:
            return
        for dy in (2, 1, -1, 0):
            home = (y + dy + NY) % NY
            send(
                "parts", parts.at[o, tp_of(dy, True)], parts_in.at[o, home], recv_part.at[o],
                (sp, tp_of(0, True)),
            )

    from_partner = set()

    def chip_sum(o, dy):
        home = (y + dy + NY) % NY
        if o not in from_partner:
            arrived(parts_in.at[o], recv_part.at[o])
            from_partner.add(o)
        return parts[o, tp_of(dy)].astype(jnp.float32) + parts_in[o, home].astype(jnp.float32)

    def reduce_far(o):
        near_out[o, 0] = chip_sum(o, 2).astype(jnp.bfloat16)
        send("far", near_out.at[o, 0, pl.ds(0, 16)], far_in.at[o, 0], recv_far.at[o, 0], (sp, tp_of(1)))
        send("far", near_out.at[o, 0, pl.ds(16, 16)], far_in.at[o, 1], recv_far.at[o, 1], (sp, tp_of(-1)))

    def reduce_near(o, n):
        dy = (1, -1)[n]
        mine = chip_sum(o, dy)
        arrived(far_in.at[o, n], recv_far.at[o, n])
        at = slice(16 * n, 16 * n + 16)
        rest = slice(16 - 16 * n, 32 - 16 * n)
        near_out[o, 1 + n, at, :] = (mine[at] + far_in[o, n].astype(jnp.float32)).astype(
            jnp.bfloat16
        )
        near_out[o, 1 + n, rest, :] = mine[rest].astype(jnp.bfloat16)
        send("near", near_out.at[o, 1 + n], near_in.at[o, n], recv_near.at[o, n], (sp, tp_of(dy)))

    def give_back(o):
        whole = chip_sum(o, 0)
        for n in (0, 1):
            arrived(near_in.at[o, n], recv_near.at[o, n])
            whole = whole + near_in[o, n].astype(jnp.float32)
        result = whole.astype(jnp.bfloat16)
        stack = jnp.concatenate([result[:, 512 * j : 512 * (j + 1)] for j in range(4)], axis=0)
        back[o] = (
            jnp.dot(unsort, stack, preferred_element_type=jnp.float32)
            .astype(jnp.bfloat16)
            .reshape(8, 16, 512)
        )
        if o == 0:
            returned[sp] = back[0, x]
        for n in (0, 1):
            dz = BACK[2 * o + n]
            for dx in (0, 1, -1, 2):
                if (dz, dx) != (0, 0):
                    to = sp_of(dz, dx)
                    send("back", back.at[o, 4 * n + to % NX], returned.at[sp], recv_back, (to, tp))

    last_down = {}
    for kind, o, *n in EXPERT_STEPS:
        if kind == "down":
            last_down[o] = n[0]
    last_down = set(last_down.items())
    steps = dict(
        own=own, near=near, far=far, sort=sort_rows, up=up, down=down, rfar=reduce_far,
        rnear=reduce_near, back=give_back,
    )
    for kind, *args in EXPERT_STEPS:
        steps[kind](*args)

    arrived(returned.at[pl.ds(0, N_SP - 1)], recv_back)
    results = returned[...].reshape(512, 512)
    routed = jnp.dot(
        merge, results.astype(jnp.float32), preferred_element_type=jnp.float32,
        precision=lax.Precision.HIGHEST,
    )
    for j in range(4):
        cols = slice(512 * j, 512 * (j + 1))
        out_ref[:, cols] = (middle_ref[:, cols] + routed[32 * j : 32 * (j + 1)]).astype(jnp.bfloat16)
    for kind, ref in (
        ("A", kv.at[pl.ds(0, N_SP - 1), pl.ds(0, ROWS_A)]),
        ("B", kv.at[pl.ds(0, N_SP - 1), pl.ds(ROWS_A, SEQ - ROWS_A)]),
        ("w", wfull.at[pl.ds(0, N_TP - 1)]),
        ("att", att_in.at[pl.ds(0, N_TP - 1)]),
        ("slots", slots.at[pl.ds(0, N_SP - 1)]),
        ("rows", rows_in.at[pl.ds(0, N_TP - 1)]),
        ("parts", parts.at[pl.ds(0, 2)]),
        ("far", parts_in.at[0]),
        ("near", parts_in.at[pl.ds(0, 2)]),
        ("back", returned.at[pl.ds(0, N_SP - 1)]),
    ):
        all_sent(kind, ref)


def local(
    x_resid,
    query_proj,
    projected_key_heads,
    projected_value_heads,
    query_gain,
    key_norm_gain,
    out_weight,
    ffn_gain,
    routing,
    route_scores,
    expert_gate,
    expert_up,
    expert_down,
):
    hbm = pl.BlockSpec(memory_space=pltpu.HBM)
    bf16, f32 = jnp.bfloat16, jnp.float32
    dma = pltpu.SemaphoreType.DMA
    return pl.pallas_call(
        layer_kernel,
        out_shape=jax.ShapeDtypeStruct((32, 2048), bf16),
        in_specs=[hbm] * 14,
        out_specs=pl.BlockSpec(memory_space=pltpu.VMEM),
        scratch_shapes=[
            pltpu.VMEM((SEQ, 256), bf16),
            pltpu.VMEM((SEQ, 128), bf16),
            pltpu.VMEM((1, 128), f32),
            pltpu.VMEM((1, 128), f32),
            pltpu.VMEM((2, 128, 128), f32),
            pltpu.VMEM((32, 2048), bf16),
            pltpu.VMEM((1, 2048), f32),
            pltpu.VMEM((2, 32), jnp.int32),
            pltpu.VMEM((2, 32), f32),
            pltpu.VMEM((2048, 512), bf16),
            pltpu.VMEM((2048, 512), bf16),
            pltpu.VMEM((512, 2048), bf16),
            pltpu.VMEM((N_SP, SEQ, 256), bf16),
            pltpu.VMEM((2, SEQ, 128), bf16),
            pltpu.VMEM((2, SEQ, 128), f32),
            pltpu.VMEM((2, SEQ, 128), f32),
            pltpu.VMEM((2, SEQ, 128), f32),
            pltpu.VMEM((N_TP, 256, 2048), bf16),
            pltpu.VMEM((SEQ, 256), bf16),
            pltpu.VMEM((N_TP, 32, 256), bf16),
            pltpu.VMEM((EXPERTS, 16, 512), bf16),
            pltpu.VMEM((N_TP, 8, NX, 16, 512), bf16),
            pltpu.VMEM((256, 2048), bf16),
            pltpu.VMEM((256, 512), bf16),
            pltpu.VMEM((4, N_TP, 32, 2048), bf16),
            pltpu.VMEM((4, NY, 32, 2048), bf16),
            pltpu.VMEM((4, 3, 32, 2048), bf16),
            pltpu.VMEM((4, 2, 16, 2048), bf16),
            pltpu.VMEM((4, 2, 32, 2048), bf16),
            pltpu.VMEM((4, 8, 16, 512), bf16),
            pltpu.VMEM((EXPERTS, 16, 512), bf16),
            pltpu.VMEM((32, 2048), f32),
            dma((len(KINDS),)),
            dma((N_SP,)),
            dma((N_SP,)),
            dma((N_TP, 2)),
            dma((N_TP,)),
            dma((14,)),
            dma((8,)),
            dma((3, 8)),
            dma((4,)),
            dma((4,)),
            dma((4, 2)),
            dma((4, 2)),
            dma,
        ],
        compiler_params=pltpu.CompilerParams(
            collective_id=0, has_side_effects=True, vmem_limit_bytes=60 * 1024 * 1024
        ),
        name="layer",
    )(
        query_proj, projected_key_heads, projected_value_heads,
        query_gain.reshape(1, -1), key_norm_gain.reshape(1, -1), turn_tables(), out_weight, x_resid,
        ffn_gain.reshape(1, -1), routing.T, route_scores.T, expert_gate, expert_up, expert_down,
    )


def solution(mesh):
    in_specs = (
        P(("sp", "tp"), None),
        P("sp", "tp"),
        P("sp", "tp"),
        P("sp", "tp"),
        P(),
        P(),
        P("tp", None),
        P(),
        P(("sp", "tp"), None),
        P(("sp", "tp"), None),
        P("sp", None, "tp"),
        P("sp", None, "tp"),
        P("sp", "tp", None),
    )
    out_specs = P(("sp", "tp"), None)
    return jax.shard_map(local, mesh=mesh, in_specs=in_specs, out_specs=out_specs, check_vma=False)
```

```python
import functools
import jax
import jax.numpy as jnp
import numpy as np
from jax import lax
from jax.experimental import pallas as pl
from jax.experimental.pallas import tpu as pltpu
from jax.sharding import PartitionSpec as P

HEAD_WIDTH = 128
TOP = 2
GRID_W = 64
NORM_EPS = 1e-06
ROPE_BASE = 10000.0
NEG_LARGE = -1e30
LOG2E = 1.4426950408889634
MESH = pl.DeviceIdType.MESH

NZ, NX, NY = 8, 4, 4
N_SP = NZ * NX
N_TP = NY * 2
SEQ = 256
ROWS_A = 96
ATTENTION_STEPS = (('A', 0, -1), ('A', 0, 1), ('B', -1, 0), ('B', 1, 0), ('A', 0, 2), ('A', -1, 0), ('A', 1, 0),
    ('B', 0, -1), ('A', -1, -1), ('A', 1, -1), ('B', 0, 1), ('A', -1, 1), ('A', 1, 1), ('B', -1, -1),
    ('B', -1, 1), ('B', -2, 0), ('B', 2, 0), ('B', 1, -1), ('A', -1, 2), ('A', 1, 2), ('B', 1, 1),
    ('A', -2, 0), ('A', 2, 0), ('B', -1, 2), ('C', -1, 0), ('A', -2, -1), ('A', 2, -1), ('B', 0, 2),
    ('C', -1, 1), ('A', -2, 1), ('A', 2, 1), ('B', -2, -1), ('C', 0, 0), ('B', -2, 1), ('C', 0, 1),
    ('B', -3, 0), ('B', 3, 0), ('B', 2, -1), ('B', 2, 1), ('A', -2, 2), ('A', 2, 2), ('B', 1, 2),
    ('C', 1, 0), ('A', 3, 0), ('A', -3, 0), ('C', 1, 1), ('A', -3, -1), ('A', 3, -1), ('B', -2, 2),
    ('C', -2, 0), ('A', 3, 1), ('B', -3, -1), ('A', -3, 1), ('C', -2, 1), ('A', -3, 2), ('B', -3, 1),
    ('B', 4, 0), ('B', 3, -1), ('B', 3, 1), ('A', 4, -1), ('A', 3, 2), ('A', 4, 0), ('B', -3, 2),
    ('B', 2, 2), ('C', -3, 0), ('A', 4, 2), ('A', 4, 1), ('C', -3, 1), ('B', 4, 1), ('B', 4, -1),
    ('C', 2, 0), ('C', 2, 1), ('B', 3, 2), ('C', 3, 0), ('C', 3, 1), ('B', 4, 2), ('C', 4, 0), ('C',
    4, 1))
EXPERT_STEPS = (('near', 0, -1), ('near', 0, 1), ('own', 0), ('own', 1), ('own', 3), ('far', 0), ('near', 1, 1),
    ('own', 4), ('near', 1, -1), ('near', 3, 1), ('own', 2), ('near', 3, -1), ('own', 5), ('far', 1),
    ('near', 4, -1), ('near', 4, 1), ('near', 2, -1), ('sort', 0), ('up', 0, 0), ('own', 6), ('far',
    3), ('up', 0, 1), ('near', 5, -1), ('down', 0, 0), ('near', 2, 1), ('down', 0, 1), ('far', 4),
    ('own', 7), ('near', 5, 1), ('far', 2), ('near', 6, 1), ('near', 6, -1), ('rfar', 0), ('sort', 1),
    ('near', 7, -1), ('near', 7, 1), ('up', 1, 0), ('up', 1, 1), ('far', 5), ('down', 1, 0), ('far',
    6), ('down', 1, 1), ('rnear', 0, 1), ('rnear', 0, 0), ('sort', 2), ('up', 2, 0), ('far', 7),
    ('up', 2, 1), ('down', 2, 0), ('rfar', 1), ('down', 2, 1), ('sort', 3), ('up', 3, 0), ('up', 3,
    1), ('back', 0), ('down', 3, 0), ('down', 3, 1), ('rfar', 2), ('rnear', 1, 0), ('rnear', 1, 1),
    ('rfar', 3), ('rnear', 2, 0), ('rnear', 2, 1), ('back', 1), ('rnear', 3, 0), ('rnear', 3, 1),
    ('back', 2), ('back', 3))


def rms_scale(values, norm_gain):
    return (
        values * lax.rsqrt(jnp.mean(values * values, axis=-1, keepdims=True) + NORM_EPS) * norm_gain
    )


EXPERTS, CAP = 32, 4
BACK = (0, 1, 2, -1, -2, -3, 3, 4)
AHEAD = (0, 1, -1, 2, -2, 3, -3, 4)
KINDS = ("A", "B", "w", "att", "slots", "rows", "parts", "far", "near", "back")


def turn_tables():
    freq_count = HEAD_WIDTH // 4
    frequency = np.power(ROPE_BASE, -np.arange(freq_count) / freq_count).astype(np.float32)
    place = np.arange(N_SP * SEQ // GRID_W, dtype=np.float32)
    angles = np.tile(place[:, None] * frequency, (1, 4)).astype(np.float64)
    sign = np.where((np.arange(HEAD_WIDTH) // freq_count) % 2 == 0, -1.0, 1.0)
    return jnp.asarray(np.stack([np.cos(angles), np.sin(angles) * sign]).astype(np.float32))


def turned(values, gain, cos, sin):
    normed = rms_scale(values, gain)
    lane = lax.broadcasted_iota(jnp.int32, normed.shape, 1)
    partner = jnp.where(
        lane % 64 < 32, pltpu.roll(normed, 96, 1), pltpu.roll(normed, 32, 1)
    )
    return (normed * cos + partner * sin).astype(jnp.bfloat16)


def iota(shape, dim):
    return lax.broadcasted_iota(jnp.int32, shape, dim)


def layer_kernel(
    q_hbm, k_hbm, v_hbm, qg_hbm, kg_hbm, table_hbm, w_hbm, x_hbm, fg_hbm, routing_hbm, scores_hbm,
    gate_hbm, up_hbm, down_hbm,
    out_ref,
    q_ref, k_ref, qg_ref, kg_ref, table_ref, x_ref, fg_ref, routing_ref, scores_ref,
    wg, wu, wd,
    kv, qs, m_ref, l_ref, acc, wfull, att, att_in,
    slots, rows_in, xr, hidden, parts, parts_in, near_out, far_in, near_in, back, returned, middle_ref,
    send_sem, recv_a, recv_b, recv_w, recv_att, load_sem,
    recv_own, recv_y, recv_other, recv_part, recv_far, recv_near, recv_back,
):
    sp = lax.axis_index("sp")
    tp = lax.axis_index("tp")
    z, x = sp // NX, sp % NX
    y, c = tp // 2, tp % 2

    def sp_of(dz, dx):
        return ((z - dz + 2 * NZ) % NZ) * NX + (x - dx + 2 * NX) % NX

    def tp_of(dy, other=False):
        return ((y + dy + NY) % NY) * 2 + ((1 - c) if other else c)

    loads = {}
    for n, (name, src, dst) in enumerate((
        ("k", k_hbm, k_ref), ("v", v_hbm, kv.at[sp, :, pl.ds(128, 128)]), ("kg", kg_hbm, kg_ref),
        ("table", table_hbm, table_ref), ("q", q_hbm, q_ref), ("qg", qg_hbm, qg_ref),
        ("w", w_hbm, wfull.at[tp]), ("x", x_hbm, x_ref), ("fg", fg_hbm, fg_ref),
        ("routing", routing_hbm, routing_ref), ("scores", scores_hbm, scores_ref),
        ("gate", gate_hbm.at[0], wg), ("up", up_hbm.at[0], wu), ("down", down_hbm.at[0], wd),
    )):
        loads[name] = pltpu.make_async_copy(src, dst, load_sem.at[n])
        loads[name].start()

    barrier = pltpu.get_barrier_semaphore()

    friends = [(sp_of(dz, dx), tp) for dz, dx in ((1, 0), (-1, 0), (0, 1), (0, -1), (0, 2))]
    for dev in friends:
        pl.semaphore_signal(barrier, inc=1, device_id=dev, device_id_type=MESH)

    def greet_tp(i, carry):
        pl.semaphore_signal(barrier, inc=1, device_id=(sp, (tp + i) % N_TP), device_id_type=MESH)
        return carry

    lax.fori_loop(1, N_TP, greet_tp, 0)

    for name in ("k", "v", "kg", "table"):
        loads[name].wait()

    def table(which):
        lane = iota((GRID_W, 128), 1)
        cols = table_ref[which, 0:GRID_W, :]
        return jnp.concatenate(
            [
                jnp.where(lane < 64, table_ref[which, pl.ds(sp * (SEQ // GRID_W) + i, 1), :], cols)
                for i in range(SEQ // GRID_W)
            ],
            axis=0,
        )

    cos, sin = table(0), table(1)
    kv[sp, :, 0:128] = turned(k_ref[...].astype(jnp.float32), kg_ref[...], cos, sin)
    loads["q"].wait()
    loads["qg"].wait()
    for h in range(2):
        qs[h] = turned(
            q_ref[:, h * 128 : (h + 1) * 128].astype(jnp.float32), qg_ref[...], cos, sin
        )
    m_ref[...] = jnp.full(m_ref.shape, NEG_LARGE, jnp.float32)
    l_ref[...] = jnp.zeros(l_ref.shape, jnp.float32)
    acc[...] = jnp.zeros(acc.shape, jnp.float32)
    pl.semaphore_wait(barrier, len(friends) + N_TP - 1)

    def send(kind, src, dst, recv, dev):
        pltpu.make_async_remote_copy(
            src_ref=src, dst_ref=dst, send_sem=send_sem.at[KINDS.index(kind)], recv_sem=recv,
            device_id=dev, device_id_type=MESH,
        ).start()

    def arrived(ref, recv):
        pltpu.make_async_remote_copy(
            src_ref=ref, dst_ref=ref, send_sem=send_sem.at[0], recv_sem=recv,
            device_id=(sp, tp_of(0, True)), device_id_type=MESH,
        ).wait_recv()

    def all_sent(kind, ref):
        pltpu.make_async_remote_copy(
            src_ref=ref, dst_ref=ref, send_sem=send_sem.at[KINDS.index(kind)],
            recv_sem=recv_back, device_id=(sp, tp_of(0, True)), device_id_type=MESH,
        ).wait_send()

    def piece(half, owner):
        if half == "A":
            return kv.at[owner, pl.ds(0, ROWS_A)], recv_a.at[owner]
        return kv.at[owner, pl.ds(ROWS_A, SEQ - ROWS_A)], recv_b.at[owner]

    def pass_on(half, dz, dx, link):
        ref, recv = piece(half, sp_of(dz, dx))
        dev = {
            "z+": (sp_of(-1, 0), tp), "z-": (sp_of(1, 0), tp),
            "x+": (sp_of(0, -1), tp), "x-": (sp_of(0, 1), tp), "x2": (sp_of(0, 2), tp),
        }[link]
        send(half, ref, ref, recv, dev)

    def next_links(half, dz, dx):
        if half == "A":
            if dz == 0:
                return ["z+", "z-"]
            if dz in (1, 2) or (dz == 3 and dx in (0, 1)):
                return ["z+"]
            if dz in (-1, -2) or (dz == -3 and dx in (-1, 2)):
                return ["z-"]
            return []
        if dx == 0:
            along = ["z+"] if dz in (1, 2, 3) else ["z-"] if dz in (-1, -2) else []
            return along + ["x+", "x-"]
        if dx == 1 and dz % 2 == 0:
            return ["x+"]
        if dx == -1 and dz % 2 == 1:
            return ["x-"]
        return []

    def w_half(owner, half):
        return wfull.at[owner, pl.ds(half * 64, 64)], recv_w.at[owner, half]

    for half, dz, dx, link in (
        ("B", 0, 0, "z+"), ("B", 0, 0, "z-"), ("A", 0, 0, "x+"), ("A", 0, 0, "x-"),
        ("A", 0, 0, "x2"), ("B", 0, 0, "x+"), ("B", 0, 0, "x-"), ("A", 0, 0, "z+"),
        ("A", 0, 0, "z-"),
    ):
        pass_on(half, dz, dx, link)
    for n in range(4):
        for part, dev in ((n, tp_of(1)), ((n + 2) % 4, tp_of(-1))):
            dst, recv = w_half(tp, part)
            send("w", w_hbm.at[pl.ds(part * 64, 64)], dst, recv, (sp, dev))
    for part in range(4):
        dst, recv = w_half(tp, part)
        send("w", w_hbm.at[pl.ds(part * 64, 64)], dst, recv, (sp, tp_of(0, True)))

    def w_event(dy, half, links):
        ref, recv = w_half(tp_of(dy), half)
        arrived(ref, recv)
        for link in links:
            dev = tp_of(0, True) if link == 0 else tp_of(link)
            send("w", ref, ref, recv, (sp, dev))

    scale2 = HEAD_WIDTH ** (-0.5) * LOG2E

    def attend(group, i):
        block = kv[pl.ds(group * NX + 2 * i, 2)].reshape(2 * SEQ, 256)
        keys, values = block[:, 0:128], block[:, 128:256]
        for h in range(2):
            s = lax.dot_general(
                qs[h], keys, (((1,), (1,)), ((), ())), preferred_element_type=jnp.float32
            )
            m_old = m_ref[h]
            m_new = jnp.maximum(m_old, jnp.max(s, axis=1, keepdims=True))
            alpha = jnp.exp2((m_old - m_new) * scale2)
            m_all = jnp.concatenate([m_new * scale2] * 4, axis=1)
            p = jnp.exp2(s * scale2 - m_all)
            l_ref[h] = l_ref[h] * alpha + (
                (p[:, 0:128] + p[:, 128:256]) + (p[:, 256:384] + p[:, 384:512])
            )
            acc[h] = acc[h] * alpha + jnp.dot(
                p.astype(jnp.bfloat16), values, preferred_element_type=jnp.float32
            )
            m_ref[h] = m_new

    w_plan = {
        16: ((-1, 0, (1, 0)), (1, 2, (-1, 0))), 26: ((-1, 1, (1, 0)), (1, 3, (-1, 0))),
        52: ((-1, 2, (0,)), (1, 0, (0,))), 71: ((-1, 3, (0,)), (1, 1, (0,))),
    }
    for count, (half, dz, dx) in enumerate(ATTENTION_STEPS):
        if half == "C":
            attend((z - dz + NZ) % NZ, dx)
        else:
            ref, recv = piece(half, sp_of(dz, dx))
            arrived(ref, recv)
            for link in next_links(half, dz, dx):
                pass_on(half, dz, dx, link)
        for dy, w_part, links in w_plan.get(count, ()):
            w_event(dy, w_part, links)

    for h in range(2):
        total = jnp.sum(l_ref[h], axis=1, keepdims=True)
        att[:, h * 128 : (h + 1) * 128] = (acc[h] / total).astype(jnp.bfloat16)

    att_in[tp] = att[pl.ds(tp * 32, 32), :]
    for dy, other in ((0, True), (1, False), (1, True), (3, False), (3, True), (2, False), (2, True)):
        to = tp_of(dy, other)
        send("att", att.at[pl.ds(to * 32, 32)], att_in.at[tp], recv_att.at[tp], (sp, to))

    w_event(2, 0, (0,))
    w_event(2, 2, (0,))

    for name in ("routing", "scores"):
        loads[name].wait()
    expert_no = iota((EXPERTS, 32), 0)
    first = (routing_ref[0:1, :] == expert_no).astype(jnp.float32)
    second = (routing_ref[1:2, :] == expert_no).astype(jnp.float32)
    top = jnp.maximum(scores_ref[0:1, :], scores_ref[1:2, :])
    e0, e1 = jnp.exp(scores_ref[0:1, :] - top), jnp.exp(scores_ref[1:2, :] - top)
    gates = first * (e0 / (e0 + e1)) + second * (e1 / (e0 + e1))
    named = first + second
    before = (iota((32, 32), 0) < iota((32, 32), 1)).astype(jnp.bfloat16)
    rank = jnp.dot(named.astype(jnp.bfloat16), before, preferred_element_type=jnp.float32)
    slot = jnp.where(named > 0.5, rank, -1.0).astype(jnp.bfloat16)
    again = (iota((32, 128), 1) % 32 == iota((32, 128), 0)).astype(jnp.bfloat16)
    slot4 = jnp.dot(slot, again, preferred_element_type=jnp.float32).astype(jnp.bfloat16)
    gates4 = jnp.dot(
        gates, again.astype(jnp.float32), preferred_element_type=jnp.float32,
        precision=lax.Precision.HIGHEST,
    )
    spread = (iota((512, EXPERTS), 0) // 16 == iota((512, EXPERTS), 1)).astype(jnp.bfloat16)
    slot_rows = jnp.dot(spread, slot4, preferred_element_type=jnp.float32)
    row = iota((512, 128), 0)
    held = (slot_rows == (row % 4).astype(jnp.float32)) & (
        (row // 4) % 4 == iota((512, 128), 1) // 32
    )
    pick = held.astype(jnp.bfloat16)
    merge_rows = jnp.where(
        held,
        jnp.dot(
            spread.astype(jnp.float32), gates4, preferred_element_type=jnp.float32,
            precision=lax.Precision.HIGHEST,
        ),
        0.0,
    )
    merge = merge_rows.T

    for name in ("w", "x", "fg"):
        loads[name].wait()
    w_event(2, 1, (0,))
    w_event(2, 3, (0,))
    total = jnp.zeros((32, 2048), jnp.float32)
    order = [(0, False), (1, False), (3, False), (2, False), (0, True), (1, True), (3, True), (2, True)]
    for dy, other in order:
        owner = tp_of(dy, other)
        if (dy, other) != (0, False):
            arrived(att_in.at[owner], recv_att.at[owner])
        if other:
            for half in range(4):
                ref, recv = w_half(owner, half)
                arrived(ref, recv)
        part = jnp.dot(att_in[owner], wfull[owner], preferred_element_type=jnp.float32)
        total = total + part.astype(jnp.bfloat16).astype(jnp.float32)
    middle = x_ref[...].astype(jnp.float32) + total.astype(jnp.bfloat16).astype(jnp.float32)
    middle_ref[...] = middle
    normed = rms_scale(middle, fg_ref[...]).astype(jnp.bfloat16)

    stacked = jnp.concatenate([normed[:, 512 * j : 512 * (j + 1)] for j in range(4)], axis=0)
    slots[...] = (
        jnp.dot(pick, stacked, preferred_element_type=jnp.float32)
        .astype(jnp.bfloat16)
        .reshape(EXPERTS, 16, 512)
    )
    rows_in[tp, 0, x] = slots[sp]
    for dx in (0, 1, -1, 2):
        to = sp_of(0, -dx)
        for n, dy in ((0, 1), (1, -1)):
            send("rows", slots.at[to], rows_in.at[tp, 0, x], recv_y.at[n, 0], (to, tp_of(dy)))
        if dx != 0:
            send("slots", slots.at[to], rows_in.at[tp, 0, x], recv_own.at[0], (to, tp))
    for dz in AHEAD[1:]:
        for dx in (0, 1, -1, 2):
            to = sp_of(-dz, -dx)
            g = BACK.index(dz)
            send("slots", slots.at[to], rows_in.at[tp, g, x], recv_own.at[g], (to, tp))

    out_no, in_no = iota((128, 128), 0), iota((128, 128), 1)
    sort = (
        in_no == (out_no % 32 // 4) * 16 + (out_no // 32) * 4 + out_no % 4
    ).astype(jnp.bfloat16)
    out_no, in_no = in_no, out_no
    unsort = (
        in_no == (out_no % 32 // 4) * 16 + (out_no // 32) * 4 + out_no % 4
    ).astype(jnp.bfloat16)

    def spread_rows(owner, g, to_far=None):
        ref = rows_in.at[owner, g]
        if to_far is not None:
            send("rows", ref, ref, recv_y.at[2, g], (sp, tp_of(to_far)))
        send("rows", ref, ref, recv_other.at[g // 2], (sp, tp_of(0, True)))

    def own(g):
        ref = rows_in.at[tp, g]
        arrived(rows_in.at[tp, 0, pl.ds(0, 3)] if g == 0 else ref, recv_own.at[g])
        if g != 0:
            for n, dy in ((0, 1), (1, -1)):
                send("rows", ref, ref, recv_y.at[n, g], (sp, tp_of(dy)))
        spread_rows(tp, g)

    def near(g, dy):
        owner = tp_of(dy)
        arrived(rows_in.at[owner, g], recv_y.at[(1 + dy) // 2, g])
        spread_rows(owner, g, -dy if (g % 2 == 0) == (dy == -1) else None)

    def far(g):
        owner = tp_of(2)
        arrived(rows_in.at[owner, g], recv_y.at[2, g])
        spread_rows(owner, g)

    def sort_rows(o):
        arrived(rows_in.at[0], recv_other.at[o])

        for t in range(N_TP):
            block = rows_in[t, 2 * o : 2 * o + 2].reshape(128, 512)
            out = jnp.dot(sort, block, preferred_element_type=jnp.float32).astype(jnp.bfloat16)
            for j in range(4):
                xr[32 * t : 32 * t + 32, 512 * j : 512 * (j + 1)] = out[32 * j : 32 * (j + 1)]

    def up(o, n):
        if (o, n) == (0, 0):
            for name in ("gate", "up", "down"):
                loads[name].wait()
        cols = slice(256 * n, 256 * (n + 1))
        gate_part = jnp.dot(xr[...], wg[:, cols], preferred_element_type=jnp.float32)
        up_part = jnp.dot(xr[...], wu[:, cols], preferred_element_type=jnp.float32)
        hidden[:, cols] = (gate_part / (1.0 + jnp.exp(-gate_part)) * up_part).astype(jnp.bfloat16)

    def down(o, n):
        for j in (2 * n, 2 * n + 1):
            cols = slice(512 * j, 512 * (j + 1))
            part = jnp.dot(hidden[...], wd[:, cols], preferred_element_type=jnp.float32)
            parts[o, :, :, cols] = part.astype(jnp.bfloat16).reshape(N_TP, 32, 512)
        if (o, n) not in last_down:
            return
        for dy in (2, 1, -1, 0):
            home = (y + dy + NY) % NY
            send(
                "parts", parts.at[o, tp_of(dy, True)], parts_in.at[o, home], recv_part.at[o],
                (sp, tp_of(0, True)),
            )

    from_partner = set()

    def chip_sum(o, dy):
        home = (y + dy + NY) % NY
        if o not in from_partner:
            arrived(parts_in.at[o], recv_part.at[o])
            from_partner.add(o)
        return parts[o, tp_of(dy)].astype(jnp.float32) + parts_in[o, home].astype(jnp.float32)

    def reduce_far(o):
        near_out[o, 0] = chip_sum(o, 2).astype(jnp.bfloat16)
        send("far", near_out.at[o, 0, pl.ds(0, 16)], far_in.at[o, 0], recv_far.at[o, 0], (sp, tp_of(1)))
        send("far", near_out.at[o, 0, pl.ds(16, 16)], far_in.at[o, 1], recv_far.at[o, 1], (sp, tp_of(-1)))

    def reduce_near(o, n):
        dy = (1, -1)[n]
        mine = chip_sum(o, dy)
        arrived(far_in.at[o, n], recv_far.at[o, n])
        at = slice(16 * n, 16 * n + 16)
        rest = slice(16 - 16 * n, 32 - 16 * n)
        near_out[o, 1 + n, at, :] = (mine[at] + far_in[o, n].astype(jnp.float32)).astype(
            jnp.bfloat16
        )
        near_out[o, 1 + n, rest, :] = mine[rest].astype(jnp.bfloat16)
        send("near", near_out.at[o, 1 + n], near_in.at[o, n], recv_near.at[o, n], (sp, tp_of(dy)))

    def give_back(o):
        whole = chip_sum(o, 0)
        for n in (0, 1):
            arrived(near_in.at[o, n], recv_near.at[o, n])
            whole = whole + near_in[o, n].astype(jnp.float32)
        result = whole.astype(jnp.bfloat16)
        stack = jnp.concatenate([result[:, 512 * j : 512 * (j + 1)] for j in range(4)], axis=0)
        back[o] = (
            jnp.dot(unsort, stack, preferred_element_type=jnp.float32)
            .astype(jnp.bfloat16)
            .reshape(8, 16, 512)
        )
        if o == 0:
            returned[sp] = back[0, x]
        for n in (0, 1):
            dz = BACK[2 * o + n]
            for dx in (0, 1, -1, 2):
                if (dz, dx) != (0, 0):
                    to = sp_of(dz, dx)
                    send("back", back.at[o, 4 * n + to % NX], returned.at[sp], recv_back, (to, tp))

    last_down = {}
    for kind, o, *n in EXPERT_STEPS:
        if kind == "down":
            last_down[o] = n[0]
    last_down = set(last_down.items())
    steps = dict(
        own=own, near=near, far=far, sort=sort_rows, up=up, down=down, rfar=reduce_far,
        rnear=reduce_near, back=give_back,
    )
    for kind, *args in EXPERT_STEPS:
        steps[kind](*args)

    arrived(returned.at[pl.ds(0, N_SP - 1)], recv_back)
    results = returned[...].reshape(512, 512)
    routed = jnp.dot(
        merge, results.astype(jnp.float32), preferred_element_type=jnp.float32,
        precision=lax.Precision.HIGHEST,
    )
    for j in range(4):
        cols = slice(512 * j, 512 * (j + 1))
        out_ref[:, cols] = (middle_ref[:, cols] + routed[32 * j : 32 * (j + 1)]).astype(jnp.bfloat16)
    for kind, ref in (
        ("A", kv.at[pl.ds(0, N_SP - 1), pl.ds(0, ROWS_A)]),
        ("B", kv.at[pl.ds(0, N_SP - 1), pl.ds(ROWS_A, SEQ - ROWS_A)]),
        ("w", wfull.at[pl.ds(0, N_TP - 1)]),
        ("att", att_in.at[pl.ds(0, N_TP - 1)]),
        ("slots", slots.at[pl.ds(0, N_SP - 1)]),
        ("rows", rows_in.at[pl.ds(0, N_TP - 1)]),
        ("parts", parts.at[pl.ds(0, 2)]),
        ("far", parts_in.at[0]),
        ("near", parts_in.at[pl.ds(0, 2)]),
        ("back", returned.at[pl.ds(0, N_SP - 1)]),
    ):
        all_sent(kind, ref)


def local(
    x_resid,
    query_proj,
    projected_key_heads,
    projected_value_heads,
    query_gain,
    key_norm_gain,
    out_weight,
    ffn_gain,
    routing,
    route_scores,
    expert_gate,
    expert_up,
    expert_down,
):
    hbm = pl.BlockSpec(memory_space=pltpu.HBM)
    bf16, f32 = jnp.bfloat16, jnp.float32
    dma = pltpu.SemaphoreType.DMA
    return pl.pallas_call(
        layer_kernel,
        out_shape=jax.ShapeDtypeStruct((32, 2048), bf16),
        in_specs=[hbm] * 14,
        out_specs=pl.BlockSpec(memory_space=pltpu.VMEM),
        scratch_shapes=[
            pltpu.VMEM((SEQ, 256), bf16),
            pltpu.VMEM((SEQ, 128), bf16),
            pltpu.VMEM((1, 128), f32),
            pltpu.VMEM((1, 128), f32),
            pltpu.VMEM((2, 128, 128), f32),
            pltpu.VMEM((32, 2048), bf16),
            pltpu.VMEM((1, 2048), f32),
            pltpu.VMEM((2, 32), jnp.int32),
            pltpu.VMEM((2, 32), f32),
            pltpu.VMEM((2048, 512), bf16),
            pltpu.VMEM((2048, 512), bf16),
            pltpu.VMEM((512, 2048), bf16),
            pltpu.VMEM((N_SP, SEQ, 256), bf16),
            pltpu.VMEM((2, SEQ, 128), bf16),
            pltpu.VMEM((2, SEQ, 128), f32),
            pltpu.VMEM((2, SEQ, 128), f32),
            pltpu.VMEM((2, SEQ, 128), f32),
            pltpu.VMEM((N_TP, 256, 2048), bf16),
            pltpu.VMEM((SEQ, 256), bf16),
            pltpu.VMEM((N_TP, 32, 256), bf16),
            pltpu.VMEM((EXPERTS, 16, 512), bf16),
            pltpu.VMEM((N_TP, 8, NX, 16, 512), bf16),
            pltpu.VMEM((256, 2048), bf16),
            pltpu.VMEM((256, 512), bf16),
            pltpu.VMEM((4, N_TP, 32, 2048), bf16),
            pltpu.VMEM((4, NY, 32, 2048), bf16),
            pltpu.VMEM((4, 3, 32, 2048), bf16),
            pltpu.VMEM((4, 2, 16, 2048), bf16),
            pltpu.VMEM((4, 2, 32, 2048), bf16),
            pltpu.VMEM((4, 8, 16, 512), bf16),
            pltpu.VMEM((EXPERTS, 16, 512), bf16),
            pltpu.VMEM((32, 2048), f32),
            dma((len(KINDS),)),
            dma((N_SP,)),
            dma((N_SP,)),
            dma((N_TP, 4)),
            dma((N_TP,)),
            dma((14,)),
            dma((8,)),
            dma((3, 8)),
            dma((4,)),
            dma((4,)),
            dma((4, 2)),
            dma((4, 2)),
            dma,
        ],
        compiler_params=pltpu.CompilerParams(
            collective_id=0, has_side_effects=True, vmem_limit_bytes=60 * 1024 * 1024
        ),
        name="layer",
    )(
        query_proj, projected_key_heads, projected_value_heads,
        query_gain.reshape(1, -1), key_norm_gain.reshape(1, -1), turn_tables(), out_weight, x_resid,
        ffn_gain.reshape(1, -1), routing.T, route_scores.T, expert_gate, expert_up, expert_down,
    )


def solution(mesh):
    in_specs = (
        P(("sp", "tp"), None),
        P("sp", "tp"),
        P("sp", "tp"),
        P("sp", "tp"),
        P(),
        P(),
        P("tp", None),
        P(),
        P(("sp", "tp"), None),
        P(("sp", "tp"), None),
        P("sp", None, "tp"),
        P("sp", None, "tp"),
        P("sp", "tp", None),
    )
    out_specs = P(("sp", "tp"), None)
    return jax.shard_map(local, mesh=mesh, in_specs=in_specs, out_specs=out_specs, check_vma=False)
```
